512 devices in a mesh: kv: 128 (over z, x, core), tp: 4 (over y).
Axes of the slice: x: 4, y: 4, z: 16, core: 2. Of those that a mesh axis runs over, the one named last changes fastest.
Arguments:
- tokens: bfloat16 [65536, 2048], P(('kv', 'tp')), may hold values from -6 to 6
- query_weight: bfloat16 [2048, 1024], P(None, 'tp'), may hold values from -0.125 to 0.125
- latent_weight: bfloat16 [2048, 256], replicated, may hold values from -0.125 to 0.125
- key_absorb: bfloat16 [8, 128, 256], P('tp'), may hold values from -0.5 to 0.5
- query_gain: bfloat16 [256], replicated, may hold values from 0.4 to 8
- latent_gain: bfloat16 [256], replicated, may hold values from 0.4 to 8
- value_absorb: bfloat16 [8, 256, 128], P('tp'), may hold values from -0.375 to 0.375
- head_gain: bfloat16 [8, 128], P('tp'), may hold values from 0.099609375 to 1.8984375
- out_weight: bfloat16 [1024, 2048], P('tp'), may hold values from -0.1875 to 0.1875
- chosen: int32 [1024, 16], P('kv'), may hold values from 0 to 1023, as said below
Outputs:
- mixed_out: bfloat16 [65536, 2048], P(('kv', 'tp'))
The draws below stay inside these ranges and needn't reach their ends.
Inputs may be any that keep to these rules, and one draw needn't show every extreme that they name: `chosen`: entry 0 of row b is b; a row's entries are distinct. Entries 1 to 3 lie in the same aligned run of 8 block numbers as b, the other 12 in other runs. For each aligned run of 8 rows and each other aligned run of 8 block numbers, those rows together name at most one block of that run. Entries above the row's own number may occur and contribute nothing.
All inputs are finite; a program needn't handle non-finite values.
Results may differ from the reference program's by a relative error of at most 0.014.
The reference program's roundings to bfloat16 on the way count: a program that leaves them out, or rounds other values in their place, can miss the bound.
Values may be sent and summed in bfloat16 or wider, within the bound.
A program may use at most 64 MiB of HBM per device.

```python
import jax
import jax.numpy as jnp
from jax import lax

D = 2048
HEADS = 8
HEAD = 128
LATENT = 256
BLOCK = 64
TOKENS = 65536
NBLK = 1024
SPAN_BLOCKS = 8
LOCAL_PICKS = 3
REMOTE = 12
NSEL = 16
HEAD_GROUP = 2
N_TP = 4


def gain_values(key, salt):
    base = jax.random.fold_in(key, salt)
    return jnp.clip(1.0 + 0.18 * jax.random.normal(base, (LATENT,), jnp.float32), 0.4, 1.6).astype(jnp.bfloat16)


def draw_query_gain(key, part):
    return gain_values(key, 11)


def draw_latent_gain(key, part):
    return gain_values(key, 23)


def draw_chosen(key, part):
    owners = NBLK // SPAN_BLOCKS
    first_key = jax.random.fold_in(key, 101)
    second_key = jax.random.fold_in(key, 202)
    third_key = jax.random.fold_in(key, 303)
    fourth_key = jax.random.fold_in(key, 404)
    block_pick = jax.random.randint(first_key, (owners, owners), 0, SPAN_BLOCKS)
    favored = (jax.random.randint(second_key, (owners,), 0, 4) == 0).astype(jnp.int32)
    row_ids = jnp.arange(NBLK, dtype=jnp.int32)
    device_of = row_ids // SPAN_BLOCKS
    local_pos = row_ids % SPAN_BLOCKS
    local_noise = jax.random.randint(third_key, (NBLK, SPAN_BLOCKS), 0, 1 << 20)
    local_range = jnp.arange(SPAN_BLOCKS, dtype=jnp.int32)
    local_score = local_noise * SPAN_BLOCKS + local_range[None, :]
    local_score = jnp.where(local_range[None, :] == local_pos[:, None], -1, local_score)
    _, local_pick = lax.top_k(local_score, LOCAL_PICKS)
    local_ids = device_of[:, None] * SPAN_BLOCKS + local_pick.astype(jnp.int32)
    owner_range = jnp.arange(owners, dtype=jnp.int32)
    remote_noise = jax.random.randint(fourth_key, (NBLK, owners), 0, 1 << 12)
    earlier = owner_range[None, :] < device_of[:, None]
    forced = (owner_range[None, :] == device_of[:, None] - 1) | (owner_range[None, :] == device_of[:, None] - owners // 2)
    level = jnp.where(forced, 3, jnp.where(earlier, 1, 0))
    level = jnp.where(owner_range[None, :] == device_of[:, None], -1, level)
    remote_score = (level * (1 << 13) + remote_noise + favored[None, :] * (1 << 11)) * owners + owner_range[None, :]
    _, remote_pick = lax.top_k(remote_score, REMOTE)
    remote_pick = remote_pick.astype(jnp.int32)
    remote_ids = remote_pick * SPAN_BLOCKS + block_pick[device_of[:, None], remote_pick]
    return jnp.concatenate([row_ids[:, None], local_ids, remote_ids], axis=1).astype(jnp.int32)


def block_scale(rng, dims, split, least, top_value):
    factor_of = 1.0
    for position, blocks in split:
        heights = jax.random.uniform(jax.random.fold_in(jax.random.fold_in(rng, 6), position), (blocks,), jnp.float32, least / len(split), top_value / len(split))
        factor_of = factor_of * jnp.repeat(jnp.exp(heights), dims[position] // blocks).reshape((-1,) + (1,) * (len(dims) - 1 - position))
    return factor_of


def scatter_about(stream_key, dims, width, reach, split=(), kind=jnp.bfloat16):
    values = jax.random.normal(stream_key, dims, jnp.float32) * width
    if len(split) > 0:
        values = block_scale(stream_key, dims, split, -0.22, 0.18) * values
    return jnp.clip(values, min=-reach, max=reach).astype(kind)


def setup_inputs(seed: int = 0) -> dict:
    keys = jax.random.split(jax.random.key(seed), 11)
    tokens = scatter_about(keys[0], (TOKENS, D), 1.0, 6.0, ((0, 512),))
    query_weight = scatter_about(keys[1], (D, HEADS * HEAD), D ** -0.5, 0.125, ((1, 4),))
    latent_weight = scatter_about(keys[2], (D, LATENT), D ** -0.5, 0.125)
    key_absorb = scatter_about(keys[3], (HEADS, HEAD, LATENT), HEAD ** -0.5, 0.5, ((0, 4),))
    query_gain = draw_query_gain(jax.random.fold_in(keys[10], 71), 0)
    latent_gain = draw_latent_gain(jax.random.fold_in(keys[10], 71), 0)
    value_absorb = scatter_about(keys[6], (HEADS, LATENT, HEAD), LATENT ** -0.5, 0.375, ((0, 4),))
    head_gain = jnp.clip(1.0 + 0.18 * jax.random.normal(keys[7], (HEADS, HEAD), jnp.float32), 0.099609375, 1.8984375).astype(jnp.bfloat16)
    out_weight = scatter_about(keys[8], (HEADS * HEAD, D), (HEADS * HEAD) ** -0.5, 0.1875, ((0, 4),))
    chosen = draw_chosen(jax.random.fold_in(keys[10], 71), 0)
    return {"tokens": tokens, "query_weight": query_weight, "latent_weight": latent_weight, "key_absorb": key_absorb, "query_gain": query_gain, "latent_gain": latent_gain, "value_absorb": value_absorb, "head_gain": head_gain, "out_weight": out_weight, "chosen": chosen}


epsilon = 1e-06

def normalize(values, gain):
    return values * lax.rsqrt(lax.optimization_barrier(jnp.mean(values * values, axis=-1, keepdims=True)) + epsilon) * gain

def reference(tokens, query_weight, latent_weight, key_absorb, query_gain, latent_gain, value_absorb, head_gain, out_weight, chosen):
    queries = jnp.dot(tokens, query_weight, preferred_element_type=jnp.float32).astype(jnp.bfloat16)
    latent = normalize(jnp.dot(tokens, latent_weight, preferred_element_type=jnp.float32), latent_gain.astype(jnp.float32)).astype(jnp.bfloat16)
    head_query = queries.reshape(TOKENS, HEADS, HEAD).astype(jnp.float32)
    absorbed = jnp.einsum('thd,hdc->thc', head_query, key_absorb.astype(jnp.float32))
    absorbed = normalize(absorbed, query_gain.astype(jnp.float32)).astype(jnp.bfloat16)
    key_blocks = latent.reshape(NBLK, BLOCK, LATENT)
    query_blocks = absorbed.reshape(NBLK, BLOCK, HEADS, LATENT)
    offsets = jnp.arange(BLOCK, dtype=jnp.int32)

    def attend(inputs):
        row_block, picked, block_index = inputs
        key_rows = key_blocks[picked].reshape(NSEL * BLOCK, LATENT).astype(jnp.float32)
        scores = jnp.einsum('qhc,kc->hqk', row_block.astype(jnp.float32), key_rows) * LATENT ** (-0.5)
        key_pos = (picked[:, None] * BLOCK + offsets[None, :]).reshape(NSEL * BLOCK)
        query_pos = block_index * BLOCK + offsets
        visible = key_pos[None, :] <= query_pos[:, None]
        scores = jnp.where(visible[None], scores, -jnp.inf)
        weights = lax.optimization_barrier(jax.nn.softmax(scores, axis=-1).astype(jnp.bfloat16)).astype(jnp.float32)
        return jnp.einsum('hqk,kc->qhc', weights, key_rows).astype(jnp.bfloat16)
    mixed = lax.map(attend, (query_blocks, chosen, jnp.arange(NBLK, dtype=jnp.int32)))
    mixed = mixed.reshape(TOKENS, HEADS, LATENT).astype(jnp.float32)
    values = jnp.einsum('thc,hcd->thd', mixed, value_absorb.astype(jnp.float32))
    head_out = normalize(values, head_gain.astype(jnp.float32)).astype(jnp.bfloat16).reshape(TOKENS, HEADS * HEAD)
    group_width = HEAD_GROUP * HEAD
    accumulated = jnp.zeros((TOKENS, D), jnp.float32)
    for group_index in range(N_TP):
        low = group_index * group_width
        partial_value = jnp.dot(head_out[:, low:low + group_width], out_weight[low:low + group_width], preferred_element_type=jnp.float32)
        accumulated = accumulated + lax.optimization_barrier(partial_value.astype(jnp.bfloat16)).astype(jnp.float32)
    return accumulated.astype(jnp.bfloat16)
```

```python
import functools

import jax
import jax.numpy as jnp
from jax import lax
from jax.experimental import pallas as pl
from jax.experimental.pallas import tpu as pltpu
from jax.sharding import Mesh
from jax.sharding import PartitionSpec as P

KV = ("kv_0", "kv_1", "kv_2")
KV_TP = ("kv_0", "kv_1", "kv_2", "tp")
MESH = pl.DeviceIdType.MESH
EPS = 1e-06
BF16 = jnp.bfloat16
F32 = jnp.float32
LOG2E = 1.4426950408889634


def rms(v, gain):
    return v * lax.rsqrt(jnp.mean(v * v, axis=-1, keepdims=True) + EPS) * gain


def kernel(
    dims,
    chosen,
    tokens_hbm,
    lw_hbm,
    qw_hbm,
    ka_hbm,
    va_hbm,
    ow_hbm,
    hg,
    qg,
    lg,
    out,
    *scratch,
):
    nz, nx, nc, ny, nsel, nloc = dims
    np_ = nx * nc
    sb = 2 * ny
    nr = nsel - nloc
    rsteps = nz // 2
    lsteps = nz - 1 - rsteps
    (
        tok, lw, wq, wo, ka, va, hgs, lat, span, piece0, want, wt, wts,
        xs, xr, ys, kvb, ab, kp, mix, ho,
        loc_sem, t_s, t_r, s_s, s_r, h_s, h_r, n_s, n_r, r_s, r_r, l_s, l_r,
        x_s, x_r, y_s, y_r, w1_s, w1_r, w2_s, w2_r, w3_s, w3_r,
        *ring,
    ) = scratch
    right = [piece0] + list(ring[:rsteps])
    left = [piece0] + list(ring[rsteps:])
    sh = piece0.shape[1]
    lat_w = piece0.shape[2]
    blk = sh * ny

    z = lax.axis_index("kv_0")
    x = lax.axis_index("kv_1")
    c = lax.axis_index("kv_2")
    y = lax.axis_index("tp")
    xc = x * nc + c

    def at_plane(d):
        p = lax.rem(xc + d + np_, np_)
        return {"kv_1": lax.div(p, nc), "kv_2": lax.rem(p, nc)}

    def at_y(e):
        return {"tp": lax.rem(y + e + ny, ny)}

    def at_z(d):
        return {"kv_0": lax.rem(z + d + nz, nz)}

    def at_x(d):
        return {"kv_1": lax.rem(x + d + nx, nx)}

    sent = []

    def send(src, dst, s, r, dev):
        cp = pltpu.make_async_remote_copy(
            src_ref=src, dst_ref=dst, send_sem=s, recv_sem=r,
            device_id=dev, device_id_type=MESH,
        )
        cp.start()
        sent.append(cp)

    def arrive(dst, s, r, dev):
        pltpu.make_async_remote_copy(
            src_ref=dst, dst_ref=dst, send_sem=s, recv_sem=r,
            device_id=dev, device_id_type=MESH,
        ).wait_recv()

    barrier = pltpu.get_barrier_semaphore()
    peers = [at_y(e) for e in range(1, ny)]
    peers += [at_z(1)] + ([at_z(-1)] if nz > 2 else [])
    peers += [at_plane(d) for d in range(1, np_)]
    for dev in peers:
        pl.semaphore_signal(barrier, inc=1, device_id=dev, device_id_type=MESH)

    tok_cp = pltpu.make_async_copy(tokens_hbm, tok, loc_sem.at[0])
    lw_cp = pltpu.make_async_copy(lw_hbm, lw, loc_sem.at[1])
    own_cps = [
        pltpu.make_async_copy(qw_hbm, wq.at[y], loc_sem.at[2]),
        pltpu.make_async_copy(ka_hbm, ka.at[y], loc_sem.at[3]),
        pltpu.make_async_copy(va_hbm, va.at[y], loc_sem.at[4]),
        pltpu.make_async_copy(ow_hbm, wo.at[y], loc_sem.at[5]),
    ]
    for cp in [tok_cp, lw_cp] + own_cps:
        cp.start()

    d_io = lax.broadcasted_iota(jnp.int32, (8, 128), 0)
    i_io = lax.broadcasted_iota(jnp.int32, (8, 128), 1)
    owner_of = lax.rem(z - lax.rem(i_io, nz) + nz, nz) * np_ + lax.rem(
        xc - lax.rem(d_io, np_) + np_, np_
    )
    acc = jnp.zeros((8, 128), jnp.int32)
    for row in range(sb):
        for p in range(nloc, nsel):
            v = chosen[row, p]
            acc = jnp.where(owner_of == lax.div(v, sb), lax.rem(v, sb), acc)
    for d in range(np_):
        row = jnp.broadcast_to(acc[d : d + 1], (8, 128))
        if d == 0:
            wt[0] = row
        else:
            want[d] = row

    tok_cp.wait()
    lw_cp.wait()
    values = jnp.dot(tok[...], lw[...], preferred_element_type=F32)
    latent = rms(values, lg[...].astype(F32)).astype(BF16).reshape(2, ny, sh, lat_w)
    lat[...] = latent
    span[pl.ds(2 * y, 2)] = latent
    piece0[pl.ds(2 * y, 2)] = lat[:, y]

    pl.semaphore_wait(barrier, len(peers))

    for e in range(1, ny):
        send(lat.at[:, lax.rem(y + e, ny)], piece0.at[pl.ds(2 * y, 2)], t_s.at[e], t_r.at[e], at_y(e))
    for d in range(1, np_):
        send(want.at[d], wt.at[d], n_s.at[d], n_r.at[d], at_plane(-d))
    for e in range(1, ny):
        send(lat, span.at[pl.ds(2 * y, 2)], s_s.at[e], s_r.at[e], at_y(e))
        send(hg, hgs.at[y], h_s.at[e], h_r.at[e], at_y(e))
    hgs[y] = hg[...]

    big = [(qw_hbm, wq), (ka_hbm, ka), (va_hbm, va), (ow_hbm, wo)]
    parts = 2 * nc
    px = lax.rem(x, 2)
    g_own = px * nc + c
    g_far = (1 - px) * nc + c
    g_mate = px * nc + (1 - c)
    g_far_mate = (1 - px) * nc + (1 - c)

    def rows_of(a, g, half=None):
        n = big[a][0].shape[0] // parts
        if half is None:
            return pl.ds(pl.multiple_of(g * n, n), n)
        return pl.ds(pl.multiple_of(g * n + half * (n // 2), n // 2), n // 2)

    order = [e for e in (1, ny - 1) if e >= 1] if ny > 2 else [1]
    order += [e for e in range(2, ny - 1)]
    for a in range(4):
        for e in order:
            send(
                big[a][0].at[rows_of(a, g_own)], big[a][1].at[y, rows_of(a, g_own)],
                w1_s.at[a, e], w1_r.at[a, e], at_y(e),
            )

    mate = {"kv_2": 1 - c}

    def spread(a):
        w = big[a][1]
        for e in order:
            ys_ = lax.rem(y - e + ny, ny)
            mine = w.at[ys_, rows_of(a, g_own)]
            arrive(mine, w1_s.at[a, e], w1_r.at[a, e], at_y(e))
            for half, dx in ((0, 1), (1, -1)):
                h = w.at[ys_, rows_of(a, g_own, half)]
                send(h, h, w2_s.at[a, e, half], w2_r.at[a, e, half], at_x(dx))
            if nc > 1:
                send(mine, mine, w3_s.at[a, e, 0], w3_r.at[a, e, 0], mate)

    def pass_on(a):
        w = big[a][1]
        for e in order:
            ys_ = lax.rem(y - e + ny, ny)
            for half in (0, 1):
                h = w.at[ys_, rows_of(a, g_far, half)]
                arrive(h, w2_s.at[a, e, half], w2_r.at[a, e, half], at_x(1))
            far = w.at[ys_, rows_of(a, g_far)]
            if nc > 1:
                send(far, far, w3_s.at[a, e, 1], w3_r.at[a, e, 1], mate)

    def collect(a):
        own_cps[a].wait()
        if nc > 1:
            w = big[a][1]
            for e in order:
                ys_ = lax.rem(y - e + ny, ny)
                for k, g in ((0, g_mate), (1, g_far_mate)):
                    arrive(w.at[ys_, rows_of(a, g)], w3_s.at[a, e, k], w3_r.at[a, e, k], mate)

    for e in range(1, ny):
        ys_ = lax.rem(y - e + ny, ny)
        arrive(piece0.at[pl.ds(2 * ys_, 2)], t_s.at[e], t_r.at[e], at_y(e))
    send(right[0], right[1], r_s.at[1], r_r.at[1], at_z(1))
    if lsteps:
        send(left[0], left[1], l_s.at[1], l_r.at[1], at_z(-1))
    for d in range(1, np_):
        arrive(wt.at[d], n_s.at[d], n_r.at[d], at_plane(d))
    wt_cp = pltpu.make_async_copy(wt, wts, loc_sem.at[6])
    wt_cp.start()
    wt_cp.wait()

    def select(ref, i):
        for d in range(np_):
            block = ref[wts[d, 0, i]]
            if d == 0:
                xr[i] = block
            else:
                xs[d * nz + i] = block

    groups = []

    def post(lo, n):
        k = len(groups)
        groups.append((lo, n))
        for d in range(1, np_):
            at = pl.ds(d * nz + lo, n)
            send(xs.at[at], xr.at[at], x_s.at[d, k], x_r.at[d, k], at_plane(d))

    select(piece0, 0)
    r_lo, l_hi = 0, nz
    for s in range(1, rsteps + 1):
        arrive(right[s], r_s.at[s], r_r.at[s], at_z(-1))
        if s < rsteps:
            send(right[s], right[s + 1], r_s.at[s + 1], r_r.at[s + 1], at_z(1))
        if s <= lsteps:
            arrive(left[s], l_s.at[s], l_r.at[s], at_z(1))
            if s < lsteps:
                send(left[s], left[s + 1], l_s.at[s + 1], l_r.at[s + 1], at_z(-1))
        select(right[s], s)
        if s <= lsteps:
            select(left[s], nz - s)
        if s % 2 == 0 or s >= rsteps - 1:
            post(r_lo, s + 1 - r_lo)
            r_lo = s + 1
            if s <= lsteps:
                post(nz - s, l_hi - (nz - s))
                l_hi = nz - s
        if s == max(1, rsteps - 2):
            spread(0)
            spread(1)
            spread(2)

    for k, (lo, n) in enumerate(groups):
        for d in range(1, np_):
            arrive(xr.at[pl.ds(d * nz + lo, n)], x_s.at[d, k], x_r.at[d, k], at_plane(d))

    for b in range(2):
        for e in list(range(1, ny)) + [0]:
            row = 2 * lax.rem(y + e, ny) + b
            for j in range(nr):
                o = lax.div(chosen[row, nloc + j], sb)
                i = lax.rem(z - lax.div(o, np_) + nz, nz)
                d = lax.rem(xc - lax.rem(o, np_) + np_, np_)
                block = xr[d * nz + i]
                if e == 0:
                    kvb[b, nloc + j, y] = block
                else:
                    ys[e - 1, b, j] = block
            if e:
                send(
                    ys.at[e - 1, b], kvb.at[b, pl.ds(nloc, nr), y],
                    y_s.at[e, b], y_r.at[e, b], at_y(e),
                )
    pass_on(0)
    pass_on(1)
    pass_on(2)
    spread(3)

    for e in range(1, ny):
        ys_ = lax.rem(y - e + ny, ny)
        arrive(span.at[pl.ds(2 * ys_, 2)], s_s.at[e], s_r.at[e], at_y(e))
        arrive(hgs.at[ys_], h_s.at[e], h_r.at[e], at_y(e))
    lane = lax.broadcasted_iota(jnp.int32, (8, 128), 1)
    first = ((z * nx + x) * nc + c) * sb
    for b in range(2):
        row = 2 * y + b
        for p in range(nloc):
            kvb[b, p] = span[lax.rem(chosen[row, p], sb)]
        for p in range(0, nsel, 2):
            base = jnp.where(lane < blk, chosen[row, p] * blk, chosen[row, p + 1] * blk - blk)
            kp[b, :, p * blk : (p + 2) * blk] = base + lane

    collect(0)
    collect(1)

    def project(g, _):
        q = jnp.dot(tok[...], wq[g], preferred_element_type=F32).astype(BF16)
        for hh in range(2):
            a = jnp.dot(q[:, hh * 128 : (hh + 1) * 128], ka[g, hh * 128 : (hh + 1) * 128, :], preferred_element_type=F32)
            a = rms(a, qg[...].astype(F32)).astype(BF16)
            at = pl.ds(pl.multiple_of((2 * g + hh) * blk, blk), blk)
            ab[0, at] = a[:blk]
            ab[1, at] = a[blk:]
        return 0

    lax.fori_loop(0, ny, project, 0)
    pass_on(3)
    collect(2)

    chunk = min(4, 2 * ny) * blk
    for b in range(2):
        for e in range(1, ny):
            ys_ = lax.rem(y - e + ny, ny)
            arrive(kvb.at[b, pl.ds(nloc, nr), ys_], y_s.at[e, b], y_r.at[e, b], at_y(e))
        keys = kvb[b].reshape(nsel * blk, lat_w)
        q_pos = (first + 2 * y + b) * blk + lax.rem(
            lax.broadcasted_iota(jnp.int32, (chunk, nsel * blk), 0), blk
        )
        seen = kp[b, 0:1, :] <= q_pos
        for i in range(2 * ny * blk // chunk):
            sc = lax.dot_general(
                ab[b, i * chunk : (i + 1) * chunk], keys, (((1,), (1,)), ((), ())),
                preferred_element_type=F32,
            )
            sc = jnp.where(seen, sc, -jnp.inf)
            top = jnp.max(sc, axis=-1, keepdims=True)
            ex = jnp.exp2((sc - top) * (LOG2E * lat_w ** (-0.5)))
            wgt = (ex * (1.0 / jnp.sum(ex, axis=-1, keepdims=True))).astype(BF16)
            mix[i * chunk : (i + 1) * chunk] = jnp.dot(
                wgt, keys, preferred_element_type=F32
            ).astype(BF16)
        for h in range(2 * ny):
            v = jnp.dot(
                mix[h * blk : (h + 1) * blk],
                va[h // 2, (h % 2) * lat_w : (h % 2 + 1) * lat_w, :],
                preferred_element_type=F32,
            )
            gain = hgs[h // 2, h % 2 : h % 2 + 1].astype(F32)
            ho[b * blk : (b + 1) * blk, h * 128 : (h + 1) * 128] = rms(v, gain).astype(BF16)

    collect(3)
    wide = min(512, out.shape[1])

    def finish(t, _):
        at = pl.ds(pl.multiple_of(t * wide, wide), wide)
        total = jnp.zeros((2 * blk, wide), F32)
        for g in range(ny):
            part = jnp.dot(ho[:, g * 256 : (g + 1) * 256], wo[g, :, at], preferred_element_type=F32)
            total = total + part.astype(BF16).astype(F32)
        out[:, at] = total.astype(BF16)
        return 0

    lax.fori_loop(0, out.shape[1] // wide, finish, 0)
    for cp in sent:
        cp.wait_send()


def body(dims, tokens, query_weight, latent_weight, key_absorb, query_gain, latent_gain, value_absorb, head_gain, out_weight, chosen):
    nz, nx, nc, ny, nsel, nloc = dims
    np_, sb, nr = nx * nc, 2 * ny, nsel - nloc
    rows, d = tokens.shape
    heads, hd, lat_w = key_absorb.shape
    blk = rows // 2
    sh = blk // ny
    any_ = pl.BlockSpec(memory_space=pl.ANY)
    vm = pl.BlockSpec(memory_space=pltpu.VMEM)
    dma = pltpu.SemaphoreType.DMA
    piece = pltpu.VMEM((sb, sh, lat_w), BF16)
    scratch = [
        pltpu.VMEM((rows, d), BF16),
        pltpu.VMEM((d, lat_w), BF16),
        pltpu.VMEM((ny, d, heads * hd), BF16),
        pltpu.VMEM((ny, heads * hd, d), BF16),
        pltpu.VMEM((ny, heads * hd, lat_w), BF16),
        pltpu.VMEM((ny, heads * lat_w, hd), BF16),
        pltpu.VMEM((ny, heads, hd), BF16),
        pltpu.VMEM((2, ny, sh, lat_w), BF16),
        pltpu.VMEM((sb, ny, sh, lat_w), BF16),
        piece,
        pltpu.VMEM((np_, 8, 128), jnp.int32),
        pltpu.VMEM((np_, 8, 128), jnp.int32),
        pltpu.SMEM((np_, 8, 128), jnp.int32),
        pltpu.VMEM((np_ * nz, sh, lat_w), BF16),
        pltpu.VMEM((np_ * nz, sh, lat_w), BF16),
        pltpu.VMEM((ny - 1, 2, nr, sh, lat_w), BF16),
        pltpu.VMEM((2, nsel, ny, sh, lat_w), BF16),
        pltpu.VMEM((2, 2 * ny * blk, lat_w), BF16),
        pltpu.VMEM((2, 8, nsel * blk), jnp.int32),
        pltpu.VMEM((2 * ny * blk, lat_w), BF16),
        pltpu.VMEM((rows, heads * ny * hd), BF16),
        dma((7,)),
        dma((ny,)), dma((ny,)), dma((ny,)), dma((ny,)), dma((ny,)), dma((ny,)),
        dma((np_,)), dma((np_,)),
        dma((nz,)), dma((nz,)), dma((nz,)), dma((nz,)),
        dma((np_, 10)), dma((np_, 10)),
        dma((ny, 2)), dma((ny, 2)),
        dma((4, ny)), dma((4, ny)),
        dma((4, ny, 2)), dma((4, ny, 2)),
        dma((4, ny, 2)), dma((4, ny, 2)),
    ] + [piece] * (nz - 1)
    return pl.pallas_call(
        functools.partial(kernel, dims),
        out_shape=jax.ShapeDtypeStruct((rows, d), BF16),
        in_specs=[pl.BlockSpec(memory_space=pltpu.SMEM)] + [any_] * 6 + [vm] * 3,
        out_specs=vm,
        scratch_shapes=scratch,
        compiler_params=pltpu.CompilerParams(
            collective_id=0, has_side_effects=True, vmem_limit_bytes=60 * 2**20
        ),
        name="attend",
    )(
        chosen,
        tokens,
        latent_weight,
        query_weight,
        key_absorb.reshape(heads * hd, lat_w),
        value_absorb.reshape(heads * lat_w, hd),
        out_weight,
        head_gain,
        query_gain.reshape(1, lat_w),
        latent_gain.reshape(1, lat_w),
    )


def build(devices, dims):
    nz, nx, nc, ny = dims[:4]
    finer = Mesh(devices.reshape(nz, nx, nc, ny), KV_TP)
    in_specs = (
        P(KV_TP, None),
        P(None, "tp"),
        P(),
        P("tp", None, None),
        P(),
        P(),
        P("tp", None, None),
        P("tp", None),
        P("tp", None),
        P(KV, None),
    )
    return jax.shard_map(
        functools.partial(body, dims), mesh=finer, in_specs=in_specs, out_specs=P(KV_TP, None), check_vma=False
    )


def solution(mesh):
    return build(mesh.devices, (16, 4, 2, mesh.shape["tp"], 16, 4))
```

```python
import functools

import jax
import jax.numpy as jnp
from jax import lax
from jax.experimental import pallas as pl
from jax.experimental.pallas import tpu as pltpu
from jax.sharding import Mesh
from jax.sharding import PartitionSpec as P

KV = ("kv_0", "kv_1", "kv_2")
KV_TP = ("kv_0", "kv_1", "kv_2", "tp")
MESH = pl.DeviceIdType.MESH
EPS = 1e-06
BF16 = jnp.bfloat16
F32 = jnp.float32
LOG2E = 1.4426950408889634
CUTS = 4


def rms(v, gain):
    return v * lax.rsqrt(jnp.mean(v * v, axis=-1, keepdims=True) + EPS) * gain


def kernel(
    dims,
    chosen_hbm,
    tokens_hbm,
    lw_hbm,
    qw_hbm,
    ka_hbm,
    va_hbm,
    ow_hbm,
    hg,
    qg_hbm,
    lg_hbm,
    out,
    *scratch,
):
    nz, nx, nc, ny, nsel, nloc = dims
    np_ = nx * nc
    sb = 2 * ny
    nr = nsel - nloc
    rsteps = nz // 2
    lsteps = nz - 1 - rsteps
    (
        chosen, qg, lg, tok, lw, wq, wo, ka, va, hgs, lat, span, piece0, want, wt, wts,
        xs, xr, ys, kvb, ab, kp, mix, ho,
        loc_sem, small_s, small_r, r_s, r_r, l_s, l_r,
        x_s, x_r, y_s, y_r, w_s, w1_r, w2_r, w3_r,
        *ring,
    ) = scratch
    right = [piece0] + list(ring[:rsteps])
    left = [piece0] + list(ring[rsteps:])
    sh = piece0.shape[1]
    lat_w = piece0.shape[2]
    blk = sh * ny

    z = lax.axis_index("kv_0")
    x = lax.axis_index("kv_1")
    c = lax.axis_index("kv_2")
    y = lax.axis_index("tp")
    xc = x * nc + c

    def at_plane(d):
        p = lax.rem(xc + d + np_, np_)
        return {"kv_1": lax.div(p, nc), "kv_2": lax.rem(p, nc)}

    def at_y(e):
        return {"tp": lax.rem(y + e + ny, ny)}

    def at_z(d):
        return {"kv_0": lax.rem(z + d + nz, nz)}

    def at_x(d):
        return {"kv_1": lax.rem(x + d + nx, nx)}

    def when(cond, f):
        if cond is None:
            f()
        else:
            pl.when(cond)(f)

    def remote(src, dst, s, r, dev):
        return pltpu.make_async_remote_copy(
            src_ref=src, dst_ref=dst, send_sem=s, recv_sem=r,
            device_id=dev, device_id_type=MESH,
        )

    def send(src, dst, s, r, dev, cond=None):
        when(cond, remote(src, dst, s, r, dev).start)

    def arrive(ref, r, cond=None):
        when(cond, remote(ref, ref, loc_sem.at[0], r, at_y(1)).wait_recv)

    drains = []

    def drain(ref, s, cond=None):
        drains.append((cond, remote(ref, ref, s, loc_sem.at[0], at_y(1))))

    tok_cp = pltpu.make_async_copy(tokens_hbm, tok, loc_sem.at[0])
    lw_cp = pltpu.make_async_copy(lw_hbm, lw, loc_sem.at[1])
    own_cps = [
        pltpu.make_async_copy(qw_hbm, wq.at[y], loc_sem.at[2]),
        pltpu.make_async_copy(ka_hbm, ka.at[y], loc_sem.at[3]),
        pltpu.make_async_copy(va_hbm, va.at[y], loc_sem.at[4]),
        pltpu.make_async_copy(ow_hbm, wo.at[y], loc_sem.at[5]),
    ]
    small_cps = [
        pltpu.make_async_copy(chosen_hbm, chosen, loc_sem.at[7]),
        pltpu.make_async_copy(lg_hbm, lg, loc_sem.at[8]),
        pltpu.make_async_copy(qg_hbm, qg, loc_sem.at[9]),
        pltpu.make_async_copy(hg, hgs.at[y], loc_sem.at[10]),
    ]
    for cp in small_cps + [tok_cp, lw_cp] + own_cps:
        cp.start()

    xs[...] = jnp.zeros_like(xs)
    xr[...] = jnp.zeros_like(xr)

    barrier = pltpu.get_barrier_semaphore()
    peers = [at_y(e) for e in range(1, ny)]
    peers += [at_z(d) for d in sorted({1 % nz, 2 % nz, (nz - 1) % nz, (nz - 2) % nz} - {0})]
    peers += [at_plane(d) for d in range(1, np_)]
    for dev in peers:
        pl.semaphore_signal(barrier, inc=1, device_id=dev, device_id_type=MESH)

    d_io = lax.broadcasted_iota(jnp.int32, (8, 128), 0)
    i_io = lax.broadcasted_iota(jnp.int32, (8, 128), 1)
    owner_of = lax.rem(z - lax.rem(i_io, nz) + nz, nz) * np_ + lax.rem(
        xc - lax.rem(d_io, np_) + np_, np_
    )
    acc = jnp.zeros((8, 128), jnp.int32)
    small_cps[0].wait()
    for row in range(sb):
        for p in range(nloc, nsel):
            v = chosen[row, p]
            acc = jnp.where(owner_of == lax.div(v, sb), lax.rem(v, sb), acc)
    for d in range(np_):
        row = jnp.broadcast_to(acc[d : d + 1], (8, 128))
        if d == 0:
            wt[0] = row
        else:
            want[d] = row

    small_cps[1].wait()
    tok_cp.wait()
    lw_cp.wait()
    values = jnp.dot(tok[...], lw[...], preferred_element_type=F32)
    latent = rms(values, lg[...].astype(F32).reshape(1, lat_w)).astype(BF16).reshape(2, ny, sh, lat_w)
    lat[...] = latent
    span[pl.ds(2 * y, 2)] = latent
    piece0[pl.ds(2 * y, 2)] = lat[:, y]

    pl.semaphore_wait(barrier, len(peers))

    for e in range(1, ny):
        send(lat.at[:, lax.rem(y + e, ny)], piece0.at[pl.ds(2 * y, 2)], small_s.at[0], small_r.at[0], at_y(e))
    for d in range(1, np_):
        send(want.at[d], wt.at[d], small_s.at[1], small_r.at[1], at_plane(-d))
    others = piece0.at[pl.ds(0, 2 * (ny - 1))]
    drain(others, small_s.at[0])
    drain(wt.at[pl.ds(1, np_ - 1)], small_s.at[1])

    big = [(qw_hbm, wq), (ka_hbm, ka), (va_hbm, va), (ow_hbm, wo)]
    parts = 2 * nc
    near = [1, ny - 1] if ny > 2 else [1]
    nj = ny - 1
    shard_of = [lax.rem(y - e + ny, ny) for e in near]
    if ny > 2:
        shard_of.append(lax.rem(y + 2, ny))
    mate = {"kv_2": 1 - c}

    def rows_of(a, far=False, half=None):
        par = lax.rem(x if a < 3 else z, 2)
        g = (1 - par if far else par) * nc + c
        n = big[a][0].shape[0] // parts
        if half is None:
            return pl.ds(pl.multiple_of(g * n, n), n)
        return pl.ds(pl.multiple_of(g * n + half * (n // 2), n // 2), n // 2)

    def shares(a, k):
        n = big[a][0].shape[0] // parts
        return big[a][1].at[pl.ds(0, nj), pl.ds(0, k * n)]

    def launch(a):
        for j, e in enumerate(near):
            send(big[a][0].at[rows_of(a)], big[a][1].at[y, rows_of(a)], w_s.at[0, a], w1_r.at[a, j], at_y(e))
        drain(shares(a, 1), w_s.at[0, a])
        drain(shares(a, 1), w_s.at[1, a])
        if nc > 1:
            drain(shares(a, 2), w_s.at[2, a])

    def forward(a):
        w = big[a][1]
        for j in range(len(near)):
            arrive(w.at[shard_of[j], rows_of(a)], w1_r.at[a, j])
            if ny > 2:
                part = w.at[shard_of[j], rows_of(a, half=j)]
                send(part, part, w_s.at[0, a], w1_r.at[a, 2], at_y(near[j]))

    def spread(a, j):
        w = big[a][1]
        mine = w.at[shard_of[j], rows_of(a)]
        if j == 2:
            arrive(mine, w1_r.at[a, 2])
        for half, d in ((0, 1), (1, -1)):
            part = w.at[shard_of[j], rows_of(a, half=half)]
            send(part, part, w_s.at[1, a], w2_r.at[a, j], at_x(d) if a < 3 else at_z(d))
        if nc > 1:
            send(mine, mine, w_s.at[2, a], w3_r.at[a, 0], mate)

    def pass_on(a):
        w = big[a][1]
        for j in range(nj):
            far = w.at[shard_of[j], rows_of(a, far=True)]
            arrive(far, w2_r.at[a, j])
            if nc > 1:
                send(far, far, w_s.at[2, a], w3_r.at[a, 1], mate)

    def collect(a):
        own_cps[a].wait()
        if nc > 1:
            arrive(shares(a, 1), w3_r.at[a, 0])
            arrive(shares(a, 1), w3_r.at[a, 1])

    for a in range(3):
        launch(a)

    arrive(others, small_r.at[0])

    def targets(s, steps):
        ts = [1] if s < 2 else ([2, 1] if s % 2 == 0 else [])
        return [t for t in ts if s + t <= steps]

    cut = sb // CUTS
    r_hops = [(s, t) for s in range(rsteps) for t in targets(s, rsteps)]
    l_hops = [(s, t) for s in range(lsteps) for t in targets(s, lsteps)]

    def r_cond(s, t):
        return jnp.logical_and(z >= s, z + t <= nz - 1)

    def l_cond(s):
        return lax.rem(z + s, nz) < lsteps

    def hop_right(s, k):
        at = pl.ds(k * cut, cut)
        for t in targets(s, rsteps):
            h = r_hops.index((s, t))
            send(right[s].at[at], right[s + t].at[at], r_s.at[h], r_r.at[s + t - 1, k], at_z(t), r_cond(s, t))

    def hop_left(s, k):
        at = pl.ds(k * cut, cut)
        for t in targets(s, lsteps):
            h = l_hops.index((s, t))
            send(left[s].at[at], left[s + t].at[at], l_s.at[h], l_r.at[s + t - 1, k], at_z(-t), l_cond(s))

    for k in range(CUTS):
        hop_right(0, k)
        hop_left(0, k)
    for h, (s, t) in enumerate(r_hops):
        drain(right[s], r_s.at[h], r_cond(s, t))
    for h, (s, t) in enumerate(l_hops):
        drain(left[s], l_s.at[h], l_cond(s))

    for e in range(1, ny):
        send(lat, span.at[pl.ds(2 * y, 2)], small_s.at[2], small_r.at[2], at_y(e))
        send(hg, hgs.at[y], small_s.at[3], small_r.at[3], at_y(e))
    drain(span.at[pl.ds(0, 2 * (ny - 1))], small_s.at[2])
    drain(hgs.at[pl.ds(0, ny - 1)], small_s.at[3])

    arrive(wt.at[pl.ds(1, np_ - 1)], small_r.at[1])
    wt_cp = pltpu.make_async_copy(wt, wts, loc_sem.at[6])
    wt_cp.start()
    wt_cp.wait()

    def select(ref, i):
        for d in range(np_):
            block = ref[wts[d, 0, i]]
            if d == 0:
                xr[i] = block
            else:
                xs[d * nz + i] = block

    groups = []

    def post(lo, n, cond):
        k = len(groups)
        groups.append((n, cond))
        for d in range(1, np_):
            at = pl.ds(d * nz + lo, n)
            send(xs.at[at], xr.at[at], x_s.at[k], x_r.at[k], at_plane(d), cond)
        drain(xs.at[pl.ds(0, (np_ - 1) * n)], x_s.at[k], cond)

    def take(s):
        for k in range(CUTS):
            at = pl.ds(k * cut, cut)
            arrive(right[s].at[at], r_r.at[s - 1, k], z >= s)
            if s < rsteps:
                hop_right(s, k)
            if s <= lsteps:
                arrive(left[s].at[at], l_r.at[s - 1, k], l_cond(s))
                if s < lsteps:
                    hop_left(s, k)

    select(piece0, 0)
    r_lo, l_hi = 0, nz
    stages = [[1], [2]] + [[s + 1, s] for s in range(3, nz, 2)]
    for stage in stages:
        stage = [s for s in stage if s <= rsteps]
        if not stage:
            continue
        for s in stage:
            take(s)
        for s in stage:
            pl.when(z >= s)(functools.partial(select, right[s], s))
            if s <= lsteps:
                pl.when(z + s >= nz)(functools.partial(select, left[s], nz - s))
        top = max(stage)
        if top > 1 or top == rsteps:
            post(r_lo, top + 1 - r_lo, z >= r_lo)
            r_lo = top + 1
            l_top = min(top, lsteps)
            if nz - l_top < l_hi:
                post(nz - l_top, l_hi - (nz - l_top), z + l_top >= nz)
                l_hi = nz - l_top
        if 1 in stage:
            forward(0)
            for j in range(len(near)):
                spread(0, j)
        if 2 in stage or rsteps < 2:
            for a in (1, 2):
                forward(a)
                for j in range(len(near)):
                    spread(a, j)
            launch(3)
        if 4 in stage:
            for a in range(3):
                if nj > 2:
                    spread(a, 2)
        if 6 in stage:
            forward(3)
    if rsteps < 4 and nj > 2:
        for a in range(3):
            spread(a, 2)
    if rsteps < 6:
        forward(3)
    for j in range(len(near)):
        spread(3, j)
    for a in range(3):
        pass_on(a)
    if nj > 2:
        spread(3, 2)

    for k, (n, cond) in enumerate(groups):
        arrive(xr.at[pl.ds(0, (np_ - 1) * n)], x_r.at[k], cond)

    for b in range(2):
        for e in list(range(1, ny)) + [0]:
            row = 2 * lax.rem(y + e, ny) + b
            for j in range(nr):
                o = lax.div(chosen[row, nloc + j], sb)
                i = lax.rem(z - lax.div(o, np_) + nz, nz)
                d = lax.rem(xc - lax.rem(o, np_) + np_, np_)
                block = xr[d * nz + i]
                if e == 0:
                    kvb[b, nloc + j, y] = block
                else:
                    ys[e - 1, b, j] = block
            if e:
                send(ys.at[e - 1, b], kvb.at[b, pl.ds(nloc, nr), y], y_s.at[b], y_r.at[b], at_y(e))
        drain(ys.at[:, b], y_s.at[b])
    arrive(span.at[pl.ds(0, 2 * (ny - 1))], small_r.at[2])
    arrive(hgs.at[pl.ds(0, ny - 1)], small_r.at[3])
    lane = lax.broadcasted_iota(jnp.int32, (8, 128), 1)
    first = ((z * nx + x) * nc + c) * sb
    for b in range(2):
        row = 2 * y + b
        for p in range(nloc):
            kvb[b, p] = span[lax.rem(chosen[row, p], sb)]
        for p in range(0, nsel, 2):
            base = jnp.where(lane < blk, chosen[row, p] * blk, chosen[row, p + 1] * blk - blk)
            kp[b, :, p * blk : (p + 2) * blk] = base + lane

    small_cps[2].wait()
    small_cps[3].wait()
    collect(0)
    collect(1)

    def project(g, _):
        q = jnp.dot(tok[...], wq[g], preferred_element_type=F32).astype(BF16)
        for hh in range(2):
            a = jnp.dot(q[:, hh * 128 : (hh + 1) * 128], ka[g, hh * 128 : (hh + 1) * 128, :], preferred_element_type=F32)
            a = rms(a, qg[...].astype(F32).reshape(1, lat_w)).astype(BF16)
            at = pl.ds(pl.multiple_of((2 * g + hh) * blk, blk), blk)
            ab[0, at] = a[:blk]
            ab[1, at] = a[blk:]
        return 0

    lax.fori_loop(0, ny, project, 0)
    collect(2)

    chunk = min(4, 2 * ny) * blk
    for b in range(2):
        arrive(ys.at[:, b], y_r.at[b])
        keys = kvb[b].reshape(nsel * blk, lat_w)
        q_pos = (first + 2 * y + b) * blk + lax.rem(
            lax.broadcasted_iota(jnp.int32, (chunk, nsel * blk), 0), blk
        )
        seen = kp[b, 0:1, :] <= q_pos
        for i in range(2 * ny * blk // chunk):
            sc = lax.dot_general(
                ab[b, i * chunk : (i + 1) * chunk], keys, (((1,), (1,)), ((), ())),
                preferred_element_type=F32,
            )
            sc = jnp.where(seen, sc, -jnp.inf)
            top = jnp.max(sc, axis=-1, keepdims=True)
            ex = jnp.exp2((sc - top) * (LOG2E * lat_w ** (-0.5)))
            wgt = (ex * (1.0 / jnp.sum(ex, axis=-1, keepdims=True))).astype(BF16)
            mix[i * chunk : (i + 1) * chunk] = jnp.dot(
                wgt, keys, preferred_element_type=F32
            ).astype(BF16)
        for h in range(2 * ny):
            v = jnp.dot(
                mix[h * blk : (h + 1) * blk],
                va[h // 2, (h % 2) * lat_w : (h % 2 + 1) * lat_w, :],
                preferred_element_type=F32,
            )
            gain = hgs[h // 2, h % 2 : h % 2 + 1].astype(F32)
            ho[b * blk : (b + 1) * blk, h * 128 : (h + 1) * 128] = rms(v, gain).astype(BF16)
        if b == 0:
            pass_on(3)

    collect(3)
    wide = min(512, out.shape[1])

    def finish(t, _):
        at = pl.ds(pl.multiple_of(t * wide, wide), wide)
        total = jnp.zeros((2 * blk, wide), F32)
        for g in range(ny):
            part = jnp.dot(ho[:, g * 256 : (g + 1) * 256], wo[g, :, at], preferred_element_type=F32)
            total = total + part.astype(BF16).astype(F32)
        out[:, at] = total.astype(BF16)
        return 0

    lax.fori_loop(0, out.shape[1] // wide, finish, 0)
    for cond, cp in drains:
        when(cond, cp.wait_send)


def body(dims, tokens, query_weight, latent_weight, key_absorb, query_gain, latent_gain, value_absorb, head_gain, out_weight, chosen):
    nz, nx, nc, ny, nsel, nloc = dims
    np_, sb, nr = nx * nc, 2 * ny, nsel - nloc
    rows, d = tokens.shape
    heads, hd, lat_w = key_absorb.shape
    blk = rows // 2
    sh = blk // ny
    rsteps = nz // 2
    any_ = pl.BlockSpec(memory_space=pl.ANY)
    vm = pl.BlockSpec(memory_space=pltpu.VMEM)
    dma = pltpu.SemaphoreType.DMA
    piece = pltpu.VMEM((sb, sh, lat_w), BF16)
    scratch = [
        pltpu.SMEM((sb, nsel), jnp.int32),
        pltpu.VMEM((lat_w,), BF16),
        pltpu.VMEM((lat_w,), BF16),
        pltpu.VMEM((rows, d), BF16),
        pltpu.VMEM((d, lat_w), BF16),
        pltpu.VMEM((ny, d, heads * hd), BF16),
        pltpu.VMEM((ny, heads * hd, d), BF16),
        pltpu.VMEM((ny, heads * hd, lat_w), BF16),
        pltpu.VMEM((ny, heads * lat_w, hd), BF16),
        pltpu.VMEM((ny, heads, hd), BF16),
        pltpu.VMEM((2, ny, sh, lat_w), BF16),
        pltpu.VMEM((sb, ny, sh, lat_w), BF16),
        piece,
        pltpu.VMEM((np_, 8, 128), jnp.int32),
        pltpu.VMEM((np_, 8, 128), jnp.int32),
        pltpu.SMEM((np_, 8, 128), jnp.int32),
        pltpu.VMEM((np_ * nz, sh, lat_w), BF16),
        pltpu.VMEM((np_ * nz, sh, lat_w), BF16),
        pltpu.VMEM((ny - 1, 2, nr, sh, lat_w), BF16),
        pltpu.VMEM((2, nsel, ny, sh, lat_w), BF16),
        pltpu.VMEM((2, 2 * ny * blk, lat_w), BF16),
        pltpu.VMEM((2, 8, nsel * blk), jnp.int32),
        pltpu.VMEM((2 * ny * blk, lat_w), BF16),
        pltpu.VMEM((rows, heads * ny * hd), BF16),
        dma((11,)),
        dma((4,)), dma((4,)),
        dma((rsteps + 4,)), dma((rsteps, CUTS)), dma((rsteps + 4,)), dma((rsteps, CUTS)),
        dma((10,)), dma((10,)),
        dma((2,)), dma((2,)),
        dma((3, 4)), dma((4, 3)), dma((4, 3)), dma((4, 2)),
    ] + [piece] * (nz - 1)
    return pl.pallas_call(
        functools.partial(kernel, dims),
        out_shape=jax.ShapeDtypeStruct((rows, d), BF16),
        in_specs=[any_] * 10,
        out_specs=vm,
        scratch_shapes=scratch,
        compiler_params=pltpu.CompilerParams(
            collective_id=0, has_side_effects=True, vmem_limit_bytes=60 * 2**20
        ),
        name="attend",
    )(
        chosen,
        tokens,
        latent_weight,
        query_weight,
        key_absorb.reshape(heads * hd, lat_w),
        value_absorb.reshape(heads * lat_w, hd),
        out_weight,
        head_gain,
        query_gain,
        latent_gain,
    )


def build(devices, dims):
    nz, nx, nc, ny = dims[:4]
    finer = Mesh(devices.reshape(nz, nx, nc, ny), KV_TP)
    in_specs = (
        P(KV_TP, None),
        P(None, "tp"),
        P(),
        P("tp", None, None),
        P(),
        P(),
        P("tp", None, None),
        P("tp", None),
        P("tp", None),
        P(KV, None),
    )
    return jax.shard_map(
        functools.partial(body, dims), mesh=finer, in_specs=in_specs, out_specs=P(KV_TP, None), check_vma=False
    )


def solution(mesh):
    return build(mesh.devices, (16, 4, 2, mesh.shape["tp"], 16, 4))
```

```python
import functools

import jax
import jax.numpy as jnp
from jax import lax
from jax.experimental import pallas as pl
from jax.experimental.pallas import tpu as pltpu
from jax.sharding import Mesh
from jax.sharding import PartitionSpec as P

KV = ("kv_0", "kv_1", "kv_2")
KV_TP = ("kv_0", "kv_1", "kv_2", "tp")
MESH = pl.DeviceIdType.MESH
EPS = 1e-06
BF16 = jnp.bfloat16
F32 = jnp.float32
LOG2E = 1.4426950408889634
CUTS = 4


def rms(v, gain):
    return v * lax.rsqrt(jnp.mean(v * v, axis=-1, keepdims=True) + EPS) * gain


def kernel(
    dims,
    chosen_hbm,
    tokens_hbm,
    lw_hbm,
    qw_hbm,
    ka_hbm,
    va_hbm,
    ow_hbm,
    hg,
    qg_hbm,
    lg_hbm,
    out,
    *scratch,
):
    nz, nx, nc, ny, nsel, nloc = dims
    np_ = nx * nc
    sb = 2 * ny
    nr = nsel - nloc
    rsteps = nz // 2
    lsteps = nz - 1 - rsteps
    (
        chosen, qg, lg, tok, lw, wq, wo, ka, va, hgs, lat, span, piece0, want, wt, wts,
        xs, xr, ys, kvb, ab, kp, mix, ho,
        loc_sem, small_s, small_r, r_s, r_r, l_s, l_r,
        x_s, x_r, y_s, y_r, w_s, w1_r, w2_r, w3_r, res, out_sem, ready,
        *ring,
    ) = scratch
    right = [piece0] + list(ring[:rsteps])
    left = [piece0] + list(ring[rsteps:])
    sh = piece0.shape[1]
    lat_w = piece0.shape[2]
    blk = sh * ny

    z = lax.axis_index("kv_0")
    x = lax.axis_index("kv_1")
    c = lax.axis_index("kv_2")
    y = lax.axis_index("tp")
    xc = x * nc + c

    def at_plane(d):
        p = lax.rem(xc + d + np_, np_)
        return {"kv_1": lax.div(p, nc), "kv_2": lax.rem(p, nc)}

    def at_y(e):
        return {"tp": lax.rem(y + e + ny, ny)}

    def at_z(d):
        return {"kv_0": lax.rem(z + d + nz, nz)}

    def at_x(d):
        return {"kv_1": lax.rem(x + d + nx, nx)}

    def when(cond, f):
        if cond is None:
            f()
        else:
            pl.when(cond)(f)

    def remote(src, dst, s, r, dev):
        return pltpu.make_async_remote_copy(
            src_ref=src, dst_ref=dst, send_sem=s, recv_sem=r,
            device_id=dev, device_id_type=MESH,
        )

    def send(src, dst, s, r, dev, cond=None):
        when(cond, remote(src, dst, s, r, dev).start)

    def arrive(ref, r, cond=None):
        when(cond, remote(ref, ref, loc_sem.at[0], r, at_y(1)).wait_recv)

    drains, late = [], []

    def drain(ref, s, cond=None, to=drains):
        to.append((cond, remote(ref, ref, s, loc_sem.at[0], at_y(1))))

    def flush(queue):
        for cond, cp in queue:
            when(cond, cp.wait_send)
        queue.clear()

    split = nz > 4
    offsets = sorted({1 % nz, 2 % nz, (nz - 1) % nz, (nz - 2) % nz} - {0})
    barrier = pltpu.get_barrier_semaphore()
    peers = [(at_y(e), None) for e in range(1, ny)]
    peers += [(at_z(d), z + d < nz if split and d < 3 else None) for d in offsets]
    peers += [(at_plane(d), None) for d in range(1, np_)]

    def greet(sem, dev):
        pl.semaphore_signal(sem, inc=1, device_id=dev, device_id_type=MESH)

    for dev, cond in peers:
        when(cond, functools.partial(greet, barrier, dev))

    def enter():
        if not split:
            pl.semaphore_wait(barrier, len(peers))
            return
        for k, cond in ((0, z >= 2), (1, z == 1), (2, z == 0)):
            pl.when(cond)(functools.partial(pl.semaphore_wait, barrier, len(peers) - k))
        for d in (1, 2):
            pl.when(z + d >= nz)(functools.partial(greet, ready, at_z(d)))

    def wait_wrap():
        if split:
            pl.when(z == 0)(functools.partial(pl.semaphore_wait, ready, 2))
            pl.when(z == 1)(functools.partial(pl.semaphore_wait, ready, 1))

    tok_cp = pltpu.make_async_copy(tokens_hbm, tok, loc_sem.at[0])
    lw_cp = pltpu.make_async_copy(lw_hbm, lw, loc_sem.at[1])
    own_cps = [
        pltpu.make_async_copy(qw_hbm, wq.at[y], loc_sem.at[2]),
        pltpu.make_async_copy(ka_hbm, ka.at[y], loc_sem.at[3]),
        pltpu.make_async_copy(va_hbm, va.at[y], loc_sem.at[4]),
        pltpu.make_async_copy(ow_hbm, wo.at[y], loc_sem.at[5]),
    ]
    small_cps = [
        pltpu.make_async_copy(chosen_hbm, chosen, loc_sem.at[7]),
        pltpu.make_async_copy(lg_hbm, lg, loc_sem.at[8]),
        pltpu.make_async_copy(qg_hbm, qg, loc_sem.at[9]),
        pltpu.make_async_copy(hg, hgs.at[y], loc_sem.at[10]),
    ]
    for cp in small_cps + [tok_cp, lw_cp] + own_cps:
        cp.start()

    xs[...] = jnp.zeros_like(xs)
    xr[...] = jnp.zeros_like(xr)

    d_io = lax.broadcasted_iota(jnp.int32, (8, 128), 0)
    i_io = lax.broadcasted_iota(jnp.int32, (8, 128), 1)
    owner_of = lax.rem(z - lax.rem(i_io, nz) + nz, nz) * np_ + lax.rem(
        xc - lax.rem(d_io, np_) + np_, np_
    )
    acc = jnp.zeros((8, 128), jnp.int32)
    small_cps[0].wait()
    for row in range(sb):
        for p in range(nloc, nsel):
            v = chosen[row, p]
            acc = jnp.where(owner_of == lax.div(v, sb), lax.rem(v, sb), acc)
    for d in range(np_):
        row = jnp.broadcast_to(acc[d : d + 1], (8, 128))
        if d == 0:
            wt[0] = row
        else:
            want[d] = row

    small_cps[1].wait()
    tok_cp.wait()
    lw_cp.wait()
    values = jnp.dot(tok[...], lw[...], preferred_element_type=F32)
    latent = rms(values, lg[...].astype(F32).reshape(1, lat_w)).astype(BF16).reshape(2, ny, sh, lat_w)
    lat[...] = latent
    span[pl.ds(2 * y, 2)] = latent
    piece0[pl.ds(2 * y, 2)] = lat[:, y]

    enter()

    for e in range(1, ny):
        send(lat.at[:, lax.rem(y + e, ny)], piece0.at[pl.ds(2 * y, 2)], small_s.at[0], small_r.at[0], at_y(e))
    for d in range(1, np_):
        send(want.at[d], wt.at[d], small_s.at[1], small_r.at[1], at_plane(-d))
    others = piece0.at[pl.ds(0, 2 * (ny - 1))]
    drain(others, small_s.at[0])
    drain(wt.at[pl.ds(1, np_ - 1)], small_s.at[1])

    big = [(qw_hbm, wq), (ka_hbm, ka), (va_hbm, va), (ow_hbm, wo)]
    parts = 2 * nc
    near = [1, ny - 1] if ny > 2 else [1]
    nj = ny - 1
    shard_of = [lax.rem(y - e + ny, ny) for e in near]
    if ny > 2:
        shard_of.append(lax.rem(y + 2, ny))
    mate = {"kv_2": 1 - c}

    def rows_of(a, far=False, half=None):
        par = lax.rem(x if a < 3 else z, 2)
        g = (1 - par if far else par) * nc + c
        n = big[a][0].shape[0] // parts
        if half is None:
            return pl.ds(pl.multiple_of(g * n, n), n)
        return pl.ds(pl.multiple_of(g * n + half * (n // 2), n // 2), n // 2)

    def shares(a, k):
        n = big[a][0].shape[0] // parts
        return big[a][1].at[pl.ds(0, nj), pl.ds(0, k * n)]

    def launch(a):
        for j, e in enumerate(near):
            send(big[a][0].at[rows_of(a)], big[a][1].at[y, rows_of(a)], w_s.at[0, a], w1_r.at[a, j], at_y(e))
        drain(shares(a, 1), w_s.at[0, a], to=late)
        if a < 3:
            drain(shares(a, 1), w_s.at[1, a], to=late)
        else:
            n = big[a][0].shape[0] // parts // 2
            halves = big[a][1].at[pl.ds(0, nj), pl.ds(0, n)]
            drain(halves, w_s.at[1, a], to=late)
            drain(halves, w_s.at[3, a], z < nz - 1, to=late)
            drain(halves, w_s.at[4, a], z == 1, to=late)
        if nc > 1:
            drain(shares(a, 2), w_s.at[2, a], to=late)

    def forward(a):
        w = big[a][1]
        for j in range(len(near)):
            arrive(w.at[shard_of[j], rows_of(a)], w1_r.at[a, j])
            if ny > 2:
                part = w.at[shard_of[j], rows_of(a, half=j)]
                send(part, part, w_s.at[0, a], w1_r.at[a, 2], at_y(near[j]))

    def spread(a, j):
        w = big[a][1]
        mine = w.at[shard_of[j], rows_of(a)]
        if j == 2:
            arrive(mine, w1_r.at[a, 2])
        lo, hi = (w.at[shard_of[j], rows_of(a, half=half)] for half in (0, 1))
        if a < 3:
            send(lo, lo, w_s.at[1, a], w2_r.at[a, j], at_x(1))
            send(hi, hi, w_s.at[1, a], w2_r.at[a, j], at_x(-1))
        else:
            send(hi, hi, w_s.at[1, a], w2_r.at[a, j], at_z(-1))
            send(lo, lo, w_s.at[3, a], w2_r.at[a, j], at_z(1), z < nz - 1)
            send(lo, lo, w_s.at[4, a], w2_r.at[a, j], at_z(-1), z == 1)
        if nc > 1:
            send(mine, mine, w_s.at[2, a], w3_r.at[a, j, 0], mate)

    def pass_on(a, j):
        far = big[a][1].at[shard_of[j], rows_of(a, far=True)]
        arrive(far, w2_r.at[a, j])
        if nc > 1:
            send(far, far, w_s.at[2, a], w3_r.at[a, j, 1], mate)

    def collect(a, j):
        if nc > 1:
            slice_ = big[a][1].at[0, pl.ds(0, big[a][0].shape[0] // parts)]
            arrive(slice_, w3_r.at[a, j, 0])
            arrive(slice_, w3_r.at[a, j, 1])

    for a in range(3):
        launch(a)

    arrive(others, small_r.at[0])

    def targets(s, steps):
        ts = [1] if s < 2 else ([2, 1] if s % 2 == 0 else [])
        return [t for t in ts if s + t <= steps]

    cut = sb // CUTS
    r_hops = [(s, t) for s in range(rsteps) for t in targets(s, rsteps)]
    l_hops = [(s, t) for s in range(lsteps) for t in targets(s, lsteps)]

    def r_cond(s, t):
        return jnp.logical_and(z >= s, z + t <= nz - 1)

    def l_cond(s):
        return lax.rem(z + s, nz) < lsteps

    def hop_right(s, k):
        at = pl.ds(k * cut, cut)
        for t in targets(s, rsteps):
            h = r_hops.index((s, t))
            send(right[s].at[at], right[s + t].at[at], r_s.at[h], r_r.at[s + t - 1, k], at_z(t), r_cond(s, t))

    def hop_left(s, k, cond=None):
        at = pl.ds(k * cut, cut)
        for t in targets(s, lsteps):
            h = l_hops.index((s, t))
            ok = l_cond(s) if cond is None else cond
            send(left[s].at[at], left[s + t].at[at], l_s.at[h], l_r.at[s + t - 1, k], at_z(-t), ok)

    for k in range(CUTS):
        hop_right(0, k)
        hop_left(0, k, jnp.logical_and(l_cond(0), z > 0) if split else None)
    for h, (s, t) in enumerate(r_hops):
        drain(right[s], r_s.at[h], r_cond(s, t))
    for h, (s, t) in enumerate(l_hops):
        drain(left[s], l_s.at[h], l_cond(s))

    arrive(wt.at[pl.ds(1, np_ - 1)], small_r.at[1])
    wt_cp = pltpu.make_async_copy(wt, wts, loc_sem.at[6])
    wt_cp.start()
    wt_cp.wait()

    def select(ref, i):
        for d in range(np_):
            block = ref[wts[d, 0, i]]
            if d == 0:
                xr[i] = block
            else:
                xs[d * nz + i] = block

    groups = []

    def post(lo, n, cond):
        k = len(groups)
        groups.append((n, cond))
        for d in range(1, np_):
            at = pl.ds(d * nz + lo, n)
            send(xs.at[at], xr.at[at], x_s.at[k], x_r.at[k], at_plane(d), cond)
        drain(xs.at[pl.ds(0, (np_ - 1) * n)], x_s.at[k], cond)

    def take(s):
        for k in range(CUTS):
            at = pl.ds(k * cut, cut)
            arrive(right[s].at[at], r_r.at[s - 1, k], z >= s)
            if s < rsteps:
                hop_right(s, k)
            if s <= lsteps:
                arrive(left[s].at[at], l_r.at[s - 1, k], l_cond(s))
                if s < lsteps:
                    hop_left(s, k)

    early = z < nz // 2
    first_two = z < min(2, nz // 2)
    middle = jnp.logical_and(early, z >= 2)

    def spread_out():
        for j in range(len(near)):
            spread(3, j)

    def spread_two():
        for a in range(3):
            spread(a, 2)

    def first_planes():
        if nj > 2:
            spread_two()
        forward(3)
        spread_out()

    select(piece0, 0)
    wait_wrap()
    if split:
        for k in range(CUTS):
            hop_left(0, k, z == 0)
    r_lo, l_hi = 0, nz
    stages = [[1], [2]] + [[s + 1, s] for s in range(3, nz, 2)]
    for stage in stages:
        stage = [s for s in stage if s <= rsteps]
        if not stage:
            continue
        for s in stage:
            take(s)
        for s in stage:
            pl.when(z >= s)(functools.partial(select, right[s], s))
            if s <= lsteps:
                pl.when(z + s >= nz)(functools.partial(select, left[s], nz - s))
        top = max(stage)
        if top > 1 or top == rsteps:
            post(r_lo, top + 1 - r_lo, z >= r_lo)
            r_lo = top + 1
            l_top = min(top, lsteps)
            if nz - l_top < l_hi:
                post(nz - l_top, l_hi - (nz - l_top), z + l_top >= nz)
                l_hi = nz - l_top
        if 1 in stage:
            forward(0)
            for j in range(len(near)):
                spread(0, j)
        if 2 in stage or rsteps < 2:
            for a in (1, 2):
                forward(a)
                for j in range(len(near)):
                    spread(a, j)
            launch(3)
        if 4 in stage:
            pl.when(first_two)(first_planes)
            if nj > 2:
                pl.when(middle)(spread_two)
        if 6 in stage:
            pl.when(jnp.logical_not(first_two))(functools.partial(forward, 3))
            pl.when(middle)(spread_out)
    if rsteps < 4:
        pl.when(first_two)(first_planes)
        if nj > 2:
            pl.when(middle)(spread_two)
    if rsteps < 6:
        pl.when(jnp.logical_not(first_two))(functools.partial(forward, 3))
        pl.when(middle)(spread_out)
    for e in range(1, ny):
        send(lat, span.at[pl.ds(2 * y, 2)], small_s.at[2], small_r.at[2], at_y(e))
        send(hg, hgs.at[y], small_s.at[3], small_r.at[3], at_y(e))
    drain(span.at[pl.ds(0, 2 * (ny - 1))], small_s.at[2])
    drain(hgs.at[pl.ds(0, ny - 1)], small_s.at[3])

    pl.when(jnp.logical_not(early))(spread_out)
    for a in range(3):
        for j in range(len(near)):
            pass_on(a, j)
    if nj > 2:
        spread(3, 2)

    for k, (n, cond) in enumerate(groups):
        arrive(xr.at[pl.ds(0, (np_ - 1) * n)], x_r.at[k], cond)

    if nj > 2:
        pl.when(jnp.logical_not(early))(spread_two)

    for b in range(2):
        for e in list(range(1, ny)) + [0]:
            row = 2 * lax.rem(y + e, ny) + b
            for j in range(nr):
                o = lax.div(chosen[row, nloc + j], sb)
                i = lax.rem(z - lax.div(o, np_) + nz, nz)
                d = lax.rem(xc - lax.rem(o, np_) + np_, np_)
                block = xr[d * nz + i]
                if e == 0:
                    kvb[b, nloc + j, y] = block
                else:
                    ys[e - 1, b, j] = block
            if e:
                send(ys.at[e - 1, b], kvb.at[b, pl.ds(nloc, nr), y], y_s.at[b], y_r.at[b], at_y(e))
        drain(ys.at[:, b], y_s.at[b], to=late)
    arrive(span.at[pl.ds(0, 2 * (ny - 1))], small_r.at[2])
    arrive(hgs.at[pl.ds(0, ny - 1)], small_r.at[3])
    lane = lax.broadcasted_iota(jnp.int32, (8, 128), 1)
    first = ((z * nx + x) * nc + c) * sb
    for b in range(2):
        row = 2 * y + b
        for p in range(nloc):
            kvb[b, p] = span[lax.rem(chosen[row, p], sb)]
        for p in range(0, nsel, 2):
            base = jnp.where(lane < blk, chosen[row, p] * blk, chosen[row, p + 1] * blk - blk)
            kp[b, :, p * blk : (p + 2) * blk] = base + lane

    small_cps[2].wait()
    small_cps[3].wait()
    for cp in own_cps[:3]:
        cp.wait()
    for j in range(len(near)):
        for a in range(3):
            collect(a, j)

    def project(g):
        q = jnp.dot(tok[...], wq[g], preferred_element_type=F32).astype(BF16)
        for hh in range(2):
            a = jnp.dot(q[:, hh * 128 : (hh + 1) * 128], ka[g, hh * 128 : (hh + 1) * 128, :], preferred_element_type=F32)
            a = rms(a, qg[...].astype(F32).reshape(1, lat_w)).astype(BF16)
            at = pl.ds(pl.multiple_of((2 * g + hh) * blk, blk), blk)
            ab[0, at] = a[:blk]
            ab[1, at] = a[blk:]

    def project_near(i, _):
        project(lax.rem(y + ny + lax.rem(i + 1, 3) - 1, ny))
        return 0

    lax.fori_loop(0, len(near) + 1, project_near, 0)
    flush(drains)
    if nj > 2:
        for a in range(3):
            pass_on(a, 2)
        for a in range(3):
            collect(a, 2)
        project(shard_of[2])

    chunk = min(4, 2 * ny) * blk
    for b in range(2):
        arrive(ys.at[:, b], y_r.at[b])
        keys = kvb[b].reshape(nsel * blk, lat_w)
        q_pos = (first + 2 * y + b) * blk + lax.rem(
            lax.broadcasted_iota(jnp.int32, (chunk, nsel * blk), 0), blk
        )
        seen = kp[b, 0:1, :] <= q_pos
        for i in range(2 * ny * blk // chunk):
            sc = lax.dot_general(
                ab[b, i * chunk : (i + 1) * chunk], keys, (((1,), (1,)), ((), ())),
                preferred_element_type=F32,
            )
            sc = jnp.where(seen, sc, -jnp.inf)
            top = jnp.max(sc, axis=-1, keepdims=True)
            ex = jnp.exp2((sc - top) * (LOG2E * lat_w ** (-0.5)))
            wgt = (ex * (1.0 / jnp.sum(ex, axis=-1, keepdims=True))).astype(BF16)
            mix[i * chunk : (i + 1) * chunk] = jnp.dot(
                wgt, keys, preferred_element_type=F32
            ).astype(BF16)
        for h in range(2 * ny):
            v = jnp.dot(
                mix[h * blk : (h + 1) * blk],
                va[h // 2, (h % 2) * lat_w : (h % 2 + 1) * lat_w, :],
                preferred_element_type=F32,
            )
            gain = hgs[h // 2, h % 2 : h % 2 + 1].astype(F32)
            ho[b * blk : (b + 1) * blk, h * 128 : (h + 1) * 128] = rms(v, gain).astype(BF16)
        if b == 0:
            for j in range(nj):
                pass_on(3, j)

    own_cps[3].wait()
    for j in range(nj):
        collect(3, j)
    wide = min(512, out.shape[1])
    tiles = out.shape[1] // wide

    def out_cp(t):
        at = pl.ds(pl.multiple_of(t * wide, wide), wide)
        return pltpu.make_async_copy(res.at[:, at], out.at[:, at], out_sem.at[t])

    def finish(t, _):
        at = pl.ds(pl.multiple_of(t * wide, wide), wide)
        total = jnp.zeros((2 * blk, wide), F32)
        for g in range(ny):
            part = jnp.dot(ho[:, g * 256 : (g + 1) * 256], wo[g, :, at], preferred_element_type=F32)
            total = total + part.astype(BF16).astype(F32)
        res[:, at] = total.astype(BF16)
        out_cp(t).start()
        return 0

    lax.fori_loop(0, tiles, finish, 0)
    flush(late)
    for t in range(tiles):
        out_cp(t).wait()


def body(dims, tokens, query_weight, latent_weight, key_absorb, query_gain, latent_gain, value_absorb, head_gain, out_weight, chosen):
    nz, nx, nc, ny, nsel, nloc = dims
    np_, sb, nr = nx * nc, 2 * ny, nsel - nloc
    rows, d = tokens.shape
    heads, hd, lat_w = key_absorb.shape
    blk = rows // 2
    sh = blk // ny
    rsteps = nz // 2
    any_ = pl.BlockSpec(memory_space=pl.ANY)
    dma = pltpu.SemaphoreType.DMA
    piece = pltpu.VMEM((sb, sh, lat_w), BF16)
    scratch = [
        pltpu.SMEM((sb, nsel), jnp.int32),
        pltpu.VMEM((lat_w,), BF16),
        pltpu.VMEM((lat_w,), BF16),
        pltpu.VMEM((rows, d), BF16),
        pltpu.VMEM((d, lat_w), BF16),
        pltpu.VMEM((ny, d, heads * hd), BF16),
        pltpu.VMEM((ny, heads * hd, d), BF16),
        pltpu.VMEM((ny, heads * hd, lat_w), BF16),
        pltpu.VMEM((ny, heads * lat_w, hd), BF16),
        pltpu.VMEM((ny, heads, hd), BF16),
        pltpu.VMEM((2, ny, sh, lat_w), BF16),
        pltpu.VMEM((sb, ny, sh, lat_w), BF16),
        piece,
        pltpu.VMEM((np_, 8, 128), jnp.int32),
        pltpu.VMEM((np_, 8, 128), jnp.int32),
        pltpu.SMEM((np_, 8, 128), jnp.int32),
        pltpu.VMEM((np_ * nz, sh, lat_w), BF16),
        pltpu.VMEM((np_ * nz, sh, lat_w), BF16),
        pltpu.VMEM((ny - 1, 2, nr, sh, lat_w), BF16),
        pltpu.VMEM((2, nsel, ny, sh, lat_w), BF16),
        pltpu.VMEM((2, 2 * ny * blk, lat_w), BF16),
        pltpu.VMEM((2, 8, nsel * blk), jnp.int32),
        pltpu.VMEM((2 * ny * blk, lat_w), BF16),
        pltpu.VMEM((rows, heads * ny * hd), BF16),
        dma((11,)),
        dma((4,)), dma((4,)),
        dma((rsteps + 4,)), dma((rsteps, CUTS)), dma((rsteps + 4,)), dma((rsteps, CUTS)),
        dma((10,)), dma((10,)),
        dma((2,)), dma((2,)),
        dma((5, 4)), dma((4, 3)), dma((4, 3)), dma((4, 3, 2)),
        pltpu.VMEM((rows, d), BF16), dma((4,)), pltpu.SemaphoreType.REGULAR,
    ] + [piece] * (nz - 1)
    return pl.pallas_call(
        functools.partial(kernel, dims),
        out_shape=jax.ShapeDtypeStruct((rows, d), BF16),
        in_specs=[any_] * 10,
        out_specs=any_,
        scratch_shapes=scratch,
        compiler_params=pltpu.CompilerParams(
            collective_id=0, has_side_effects=True, vmem_limit_bytes=60 * 2**20
        ),
        name="attend",
    )(
        chosen,
        tokens,
        latent_weight,
        query_weight,
        key_absorb.reshape(heads * hd, lat_w),
        value_absorb.reshape(heads * lat_w, hd),
        out_weight,
        head_gain,
        query_gain,
        latent_gain,
    )


def build(devices, dims):
    nz, nx, nc, ny = dims[:4]
    finer = Mesh(devices.reshape(nz, nx, nc, ny), KV_TP)
    in_specs = (
        P(KV_TP, None),
        P(None, "tp"),
        P(),
        P("tp", None, None),
        P(),
        P(),
        P("tp", None, None),
        P("tp", None),
        P("tp", None),
        P(KV, None),
    )
    return jax.shard_map(
        functools.partial(body, dims), mesh=finer, in_specs=in_specs, out_specs=P(KV_TP, None), check_vma=False
    )


def solution(mesh):
    return build(mesh.devices, (16, 4, 2, mesh.shape["tp"], 16, 4))
```

```python
import functools

import jax
import jax.numpy as jnp
from jax import lax
from jax.experimental import pallas as pl
from jax.experimental.pallas import tpu as pltpu
from jax.sharding import Mesh
from jax.sharding import PartitionSpec as P

KV = ("kv_0", "kv_1", "kv_2")
KV_TP = ("kv_0", "kv_1", "kv_2", "tp")
MESH = pl.DeviceIdType.MESH
EPS = 1e-06
BF16 = jnp.bfloat16
F32 = jnp.float32
LOG2E = 1.4426950408889634
CUTS = 4


def rms(v, gain):
    return v * lax.rsqrt(jnp.mean(v * v, axis=-1, keepdims=True) + EPS) * gain


def kernel(
    dims,
    chosen_hbm,
    tokens_hbm,
    lw_hbm,
    qw_hbm,
    ka_hbm,
    va_hbm,
    ow_hbm,
    hg,
    qg_hbm,
    lg_hbm,
    out,
    *scratch,
):
    nz, nx, nc, ny, nsel, nloc = dims
    np_ = nx * nc
    sb = 2 * ny
    nr = nsel - nloc
    rsteps = nz // 2
    lsteps = nz - 1 - rsteps
    (
        chosen, qg, lg, tok, lw, wq, wo, ka, va, hgs, lat, span, piece0, want, wt, wts,
        xs, xr, ys, kvb, ab, kp, mix, ho,
        loc_sem, small_s, small_r, r_s, r_r, l_s, l_r,
        x_s, x_r, y_s, y_r, w_s, w1_r, w2_r, w3_r, res, out_sem, ready,
        *ring,
    ) = scratch
    right = [piece0] + list(ring[:rsteps])
    left = [piece0] + list(ring[rsteps:])
    sh = piece0.shape[1]
    lat_w = piece0.shape[2]
    blk = sh * ny

    z = lax.axis_index("kv_0")
    x = lax.axis_index("kv_1")
    c = lax.axis_index("kv_2")
    y = lax.axis_index("tp")
    xc = x * nc + c

    def at_plane(d):
        p = lax.rem(xc + d + np_, np_)
        return {"kv_1": lax.div(p, nc), "kv_2": lax.rem(p, nc)}

    def at_y(e):
        return {"tp": lax.rem(y + e + ny, ny)}

    def at_z(d):
        return {"kv_0": lax.rem(z + d + nz, nz)}

    def at_x(d):
        return {"kv_1": lax.rem(x + d + nx, nx)}

    def when(cond, f):
        if cond is None:
            f()
        else:
            pl.when(cond)(f)

    def remote(src, dst, s, r, dev):
        return pltpu.make_async_remote_copy(
            src_ref=src, dst_ref=dst, send_sem=s, recv_sem=r,
            device_id=dev, device_id_type=MESH,
        )

    def send(src, dst, s, r, dev, cond=None):
        when(cond, remote(src, dst, s, r, dev).start)

    def arrive(ref, r, cond=None):
        when(cond, remote(ref, ref, loc_sem.at[0], r, at_y(1)).wait_recv)

    drains, late = [], []

    def drain(ref, s, cond=None, to=drains):
        to.append((cond, remote(ref, ref, s, loc_sem.at[0], at_y(1))))

    def flush(queue):
        for cond, cp in queue:
            when(cond, cp.wait_send)
        queue.clear()

    split = nz > 4
    offsets = sorted({1 % nz, 2 % nz, (nz - 1) % nz, (nz - 2) % nz} - {0})
    barrier = pltpu.get_barrier_semaphore()
    peers = [(at_y(e), None) for e in range(1, ny)]
    peers += [(at_z(d), z + d < nz if split and d < 3 else None) for d in offsets]
    peers += [(at_plane(d), None) for d in range(1, np_)]

    def greet(sem, dev):
        pl.semaphore_signal(sem, inc=1, device_id=dev, device_id_type=MESH)

    for dev, cond in peers:
        when(cond, functools.partial(greet, barrier, dev))

    def enter():
        if not split:
            pl.semaphore_wait(barrier, len(peers))
            return
        for k, cond in ((0, z >= 2), (1, z == 1), (2, z == 0)):
            pl.when(cond)(functools.partial(pl.semaphore_wait, barrier, len(peers) - k))
        for d in (1, 2):
            pl.when(z + d >= nz)(functools.partial(greet, ready, at_z(d)))

    def wait_wrap():
        if split:
            pl.when(z == 0)(functools.partial(pl.semaphore_wait, ready, 2))
            pl.when(z == 1)(functools.partial(pl.semaphore_wait, ready, 1))

    tok_cp = pltpu.make_async_copy(tokens_hbm, tok, loc_sem.at[0])
    lw_cp = pltpu.make_async_copy(lw_hbm, lw, loc_sem.at[1])
    own_cps = [
        pltpu.make_async_copy(qw_hbm, wq.at[y], loc_sem.at[2]),
        pltpu.make_async_copy(ka_hbm, ka.at[y], loc_sem.at[3]),
        pltpu.make_async_copy(va_hbm, va.at[y], loc_sem.at[4]),
        pltpu.make_async_copy(ow_hbm, wo.at[y], loc_sem.at[5]),
    ]
    small_cps = [
        pltpu.make_async_copy(chosen_hbm, chosen, loc_sem.at[7]),
        pltpu.make_async_copy(lg_hbm, lg, loc_sem.at[8]),
        pltpu.make_async_copy(qg_hbm, qg, loc_sem.at[9]),
        pltpu.make_async_copy(hg, hgs.at[y], loc_sem.at[10]),
    ]
    for cp in small_cps + [tok_cp, lw_cp]:
        cp.start()

    xs[...] = jnp.zeros_like(xs)
    xr[...] = jnp.zeros_like(xr)

    d_io = lax.broadcasted_iota(jnp.int32, (8, 128), 0)
    i_io = lax.broadcasted_iota(jnp.int32, (8, 128), 1)
    owner_of = lax.rem(z - lax.rem(i_io, nz) + nz, nz) * np_ + lax.rem(
        xc - lax.rem(d_io, np_) + np_, np_
    )
    acc = jnp.zeros((8, 128), jnp.int32)
    small_cps[0].wait()
    for row in range(sb):
        for p in range(nloc, nsel):
            v = chosen[row, p]
            acc = jnp.where(owner_of == lax.div(v, sb), lax.rem(v, sb), acc)
    for d in range(np_):
        row = jnp.broadcast_to(acc[d : d + 1], (8, 128))
        if d == 0:
            wt[0] = row
        else:
            want[d] = row

    small_cps[1].wait()
    tok_cp.wait()
    lw_cp.wait()
    for cp in own_cps:
        cp.start()
    values = jnp.dot(tok[...], lw[...], preferred_element_type=F32)
    latent = rms(values, lg[...].astype(F32).reshape(1, lat_w)).astype(BF16).reshape(2, ny, sh, lat_w)
    lat[...] = latent
    span[pl.ds(2 * y, 2)] = latent
    piece0[pl.ds(2 * y, 2)] = lat[:, y]

    far_y = sorted(range(1, ny), key=lambda e: -min(e, ny - e))
    far_x = sorted(range(1, np_), key=lambda d: -min(d, np_ - d))
    enter()

    for e in far_y:
        send(lat.at[:, lax.rem(y + e, ny)], piece0.at[pl.ds(2 * y, 2)], small_s.at[0], small_r.at[0], at_y(e))
    for d in range(1, np_):
        send(want.at[d], wt.at[d], small_s.at[1], small_r.at[1], at_plane(-d))
    others = piece0.at[pl.ds(0, 2 * (ny - 1))]
    drain(others, small_s.at[0])
    drain(wt.at[pl.ds(1, np_ - 1)], small_s.at[1])

    big = [(qw_hbm, wq), (ka_hbm, ka), (va_hbm, va), (ow_hbm, wo)]
    parts = 2 * nc
    near = [1, ny - 1] if ny > 2 else [1]
    nj = ny - 1
    shard_of = [lax.rem(y - e + ny, ny) for e in near]
    if ny > 2:
        shard_of.append(lax.rem(y + 2, ny))
    mate = {"kv_2": 1 - c}

    def rows_of(a, far=False, half=None):
        par = lax.rem(x if a < 3 else z, 2)
        g = (1 - par if far else par) * nc + c
        n = big[a][0].shape[0] // parts
        if half is None:
            return pl.ds(pl.multiple_of(g * n, n), n)
        return pl.ds(pl.multiple_of(g * n + half * (n // 2), n // 2), n // 2)

    def shares(a, k):
        n = big[a][0].shape[0] // parts
        return big[a][1].at[pl.ds(0, nj), pl.ds(0, k * n)]

    def launch(a):
        for j, e in enumerate(near):
            send(big[a][0].at[rows_of(a)], big[a][1].at[y, rows_of(a)], w_s.at[0, a], w1_r.at[a, j], at_y(e))
        drain(shares(a, 1), w_s.at[0, a], to=late)
        if a < 3:
            drain(shares(a, 1), w_s.at[1, a], to=late)
        else:
            n = big[a][0].shape[0] // parts // 2
            halves = big[a][1].at[pl.ds(0, nj), pl.ds(0, n)]
            drain(halves, w_s.at[1, a], to=late)
            drain(halves, w_s.at[3, a], z < nz - 1, to=late)
            drain(halves, w_s.at[4, a], z == 1, to=late)
        if nc > 1:
            drain(shares(a, 2), w_s.at[2, a], to=late)

    def forward(a):
        w = big[a][1]
        for j in range(len(near)):
            arrive(w.at[shard_of[j], rows_of(a)], w1_r.at[a, j])
            if ny > 2:
                part = w.at[shard_of[j], rows_of(a, half=j)]
                send(part, part, w_s.at[0, a], w1_r.at[a, 2], at_y(near[j]))

    def spread(a, j):
        w = big[a][1]
        mine = w.at[shard_of[j], rows_of(a)]
        if j == 2:
            arrive(mine, w1_r.at[a, 2])
        lo, hi = (w.at[shard_of[j], rows_of(a, half=half)] for half in (0, 1))
        if a < 3:
            send(lo, lo, w_s.at[1, a], w2_r.at[a, j], at_x(1))
            send(hi, hi, w_s.at[1, a], w2_r.at[a, j], at_x(-1))
        else:
            send(hi, hi, w_s.at[1, a], w2_r.at[a, j], at_z(-1))
            send(lo, lo, w_s.at[3, a], w2_r.at[a, j], at_z(1), z < nz - 1)
            send(lo, lo, w_s.at[4, a], w2_r.at[a, j], at_z(-1), z == 1)
        if nc > 1:
            send(mine, mine, w_s.at[2, a], w3_r.at[a, j, 0], mate)

    def pass_on(a, j):
        far = big[a][1].at[shard_of[j], rows_of(a, far=True)]
        arrive(far, w2_r.at[a, j])
        if nc > 1:
            send(far, far, w_s.at[2, a], w3_r.at[a, j, 1], mate)

    def collect(a, j):
        if nc > 1:
            slice_ = big[a][1].at[0, pl.ds(0, big[a][0].shape[0] // parts)]
            arrive(slice_, w3_r.at[a, j, 0])
            arrive(slice_, w3_r.at[a, j, 1])

    for a in range(3):
        launch(a)

    arrive(others, small_r.at[0])

    def targets(s, steps):
        ts = [1] if s < 2 else ([2, 1] if s % 2 == 0 else [])
        return [t for t in ts if s + t <= steps]

    cut = sb // CUTS
    r_hops = [(s, t) for s in range(rsteps) for t in targets(s, rsteps)]
    l_hops = [(s, t) for s in range(lsteps) for t in targets(s, lsteps)]

    def r_cond(s, t):
        return jnp.logical_and(z >= s, z + t <= nz - 1)

    def l_cond(s):
        return lax.rem(z + s, nz) < lsteps

    def hop_right(s, k):
        at = pl.ds(k * cut, cut)
        for t in targets(s, rsteps):
            h = r_hops.index((s, t))
            send(right[s].at[at], right[s + t].at[at], r_s.at[h], r_r.at[s + t - 1, k], at_z(t), r_cond(s, t))

    def hop_left(s, k, cond=None):
        at = pl.ds(k * cut, cut)
        for t in targets(s, lsteps):
            h = l_hops.index((s, t))
            ok = l_cond(s) if cond is None else cond
            send(left[s].at[at], left[s + t].at[at], l_s.at[h], l_r.at[s + t - 1, k], at_z(-t), ok)

    for k in range(CUTS):
        hop_right(0, k)
        hop_left(0, k, jnp.logical_and(l_cond(0), z > 0) if split else None)
    for h, (s, t) in enumerate(r_hops):
        drain(right[s], r_s.at[h], r_cond(s, t))
    for h, (s, t) in enumerate(l_hops):
        drain(left[s], l_s.at[h], l_cond(s))

    arrive(wt.at[pl.ds(1, np_ - 1)], small_r.at[1])
    wt_cp = pltpu.make_async_copy(wt, wts, loc_sem.at[6])
    wt_cp.start()
    wt_cp.wait()

    def select(ref, i):
        for d in range(np_):
            block = ref[wts[d, 0, i]]
            if d == 0:
                xr[i] = block
            else:
                xs[d * nz + i] = block

    groups = []

    def post(lo, n, cond):
        k = len(groups)
        groups.append((n, cond))
        for d in far_x:
            at = pl.ds(d * nz + lo, n)
            send(xs.at[at], xr.at[at], x_s.at[k], x_r.at[k], at_plane(d), cond)
        drain(xs.at[pl.ds(0, (np_ - 1) * n)], x_s.at[k], cond)

    def take(s):
        for k in range(CUTS):
            at = pl.ds(k * cut, cut)
            arrive(right[s].at[at], r_r.at[s - 1, k], z >= s)
            if s < rsteps:
                hop_right(s, k)
            if s <= lsteps:
                arrive(left[s].at[at], l_r.at[s - 1, k], l_cond(s))
                if s < lsteps:
                    hop_left(s, k)

    early = z < nz // 2
    first_two = z < min(2, nz // 2)
    middle = jnp.logical_and(early, z >= 2)

    def spread_out():
        for j in range(len(near)):
            spread(3, j)

    def spread_two():
        for a in range(3):
            spread(a, 2)

    def first_planes():
        if nj > 2:
            spread_two()
        forward(3)
        spread_out()

    def first_weights():
        forward(0)
        for j in range(len(near)):
            spread(0, j)

    def pass_out():
        for j in range(len(near)):
            pass_on(3, j)

    select(piece0, 0)
    pl.when(first_two)(first_weights)
    wait_wrap()
    if split:
        for k in range(CUTS):
            hop_left(0, k, z == 0)
    r_lo, l_hi = 0, nz
    stages = [[1], [2]] + [[s + 1, s] for s in range(3, nz, 2)]
    for stage in stages:
        stage = [s for s in stage if s <= rsteps]
        if not stage:
            continue
        for s in stage:
            take(s)
        for s in stage:
            pl.when(z >= s)(functools.partial(select, right[s], s))
            if s <= lsteps:
                pl.when(z + s >= nz)(functools.partial(select, left[s], nz - s))
        top = max(stage)
        if top > 1 or top == rsteps:
            post(r_lo, top + 1 - r_lo, z >= r_lo)
            r_lo = top + 1
            l_top = min(top, lsteps)
            if nz - l_top < l_hi:
                post(nz - l_top, l_hi - (nz - l_top), z + l_top >= nz)
                l_hi = nz - l_top
        if 1 in stage:
            pl.when(jnp.logical_not(first_two))(first_weights)
        if 2 in stage or rsteps < 2:
            for a in (1, 2):
                forward(a)
                for j in range(len(near)):
                    spread(a, j)
            launch(3)
        if 4 in stage:
            pl.when(first_two)(first_planes)
            if nj > 2:
                pl.when(middle)(spread_two)
        if 6 in stage:
            pl.when(jnp.logical_not(first_two))(functools.partial(forward, 3))
            pl.when(middle)(spread_out)
    if rsteps < 4:
        pl.when(first_two)(first_planes)
        if nj > 2:
            pl.when(middle)(spread_two)
    if rsteps < 6:
        pl.when(jnp.logical_not(first_two))(functools.partial(forward, 3))
        pl.when(middle)(spread_out)
    for e in range(1, ny):
        send(lat, span.at[pl.ds(2 * y, 2)], small_s.at[2], small_r.at[2], at_y(e))
        send(hg, hgs.at[y], small_s.at[3], small_r.at[3], at_y(e))
    drain(span.at[pl.ds(0, 2 * (ny - 1))], small_s.at[2])
    drain(hgs.at[pl.ds(0, ny - 1)], small_s.at[3])

    pl.when(jnp.logical_not(early))(spread_out)
    for a in range(3):
        for j in range(len(near)):
            pass_on(a, j)
    if nj > 2:
        spread(3, 2)

    for k, (n, cond) in enumerate(groups):
        if k == max(0, len(groups) - 2) and nj > 2:
            pl.when(jnp.logical_not(early))(spread_two)
        arrive(xr.at[pl.ds(0, (np_ - 1) * n)], x_r.at[k], cond)

    for b in range(2):
        for e in far_y + [0]:
            row = 2 * lax.rem(y + e, ny) + b
            for j in range(nr):
                o = lax.div(chosen[row, nloc + j], sb)
                i = lax.rem(z - lax.div(o, np_) + nz, nz)
                d = lax.rem(xc - lax.rem(o, np_) + np_, np_)
                block = xr[d * nz + i]
                if e == 0:
                    kvb[b, nloc + j, y] = block
                else:
                    ys[e - 1, b, j] = block
            if e:
                send(ys.at[e - 1, b], kvb.at[b, pl.ds(nloc, nr), y], y_s.at[b], y_r.at[b], at_y(e))
        drain(ys.at[:, b], y_s.at[b], to=late)
    arrive(span.at[pl.ds(0, 2 * (ny - 1))], small_r.at[2])
    arrive(hgs.at[pl.ds(0, ny - 1)], small_r.at[3])
    lane = lax.broadcasted_iota(jnp.int32, (8, 128), 1)
    first = ((z * nx + x) * nc + c) * sb
    for b in range(2):
        row = 2 * y + b
        for p in range(nloc):
            kvb[b, p] = span[lax.rem(chosen[row, p], sb)]
        for p in range(0, nsel, 2):
            base = jnp.where(lane < blk, chosen[row, p] * blk, chosen[row, p + 1] * blk - blk)
            kp[b, :, p * blk : (p + 2) * blk] = base + lane

    small_cps[2].wait()
    small_cps[3].wait()
    for cp in own_cps[:3]:
        cp.wait()
    for j in range(len(near)):
        for a in range(3):
            collect(a, j)

    def project(g):
        q = jnp.dot(tok[...], wq[g], preferred_element_type=F32).astype(BF16)
        for hh in range(2):
            a = jnp.dot(q[:, hh * 128 : (hh + 1) * 128], ka[g, hh * 128 : (hh + 1) * 128, :], preferred_element_type=F32)
            a = rms(a, qg[...].astype(F32).reshape(1, lat_w)).astype(BF16)
            at = pl.ds(pl.multiple_of((2 * g + hh) * blk, blk), blk)
            ab[0, at] = a[:blk]
            ab[1, at] = a[blk:]

    def project_near(i, _):
        project(lax.rem(y + ny + lax.rem(i + 1, 3) - 1, ny))
        return 0

    lax.fori_loop(0, len(near) + 1, project_near, 0)
    flush(drains)
    pl.when(jnp.logical_not(first_two))(pass_out)
    if nj > 2:
        for a in range(3):
            pass_on(a, 2)
        for a in range(3):
            collect(a, 2)
        project(shard_of[2])

    chunk = min(4, 2 * ny) * blk
    for b in range(2):
        arrive(ys.at[:, b], y_r.at[b])
        keys = kvb[b].reshape(nsel * blk, lat_w)
        q_pos = (first + 2 * y + b) * blk + lax.rem(
            lax.broadcasted_iota(jnp.int32, (chunk, nsel * blk), 0), blk
        )
        seen = kp[b, 0:1, :] <= q_pos
        for i in range(2 * ny * blk // chunk):
            sc = lax.dot_general(
                ab[b, i * chunk : (i + 1) * chunk], keys, (((1,), (1,)), ((), ())),
                preferred_element_type=F32,
            )
            sc = jnp.where(seen, sc, -jnp.inf)
            top = jnp.max(sc, axis=-1, keepdims=True)
            ex = jnp.exp2((sc - top) * (LOG2E * lat_w ** (-0.5)))
            wgt = (ex * (1.0 / jnp.sum(ex, axis=-1, keepdims=True))).astype(BF16)
            mix[i * chunk : (i + 1) * chunk] = jnp.dot(
                wgt, keys, preferred_element_type=F32
            ).astype(BF16)
        for h in range(2 * ny):
            v = jnp.dot(
                mix[h * blk : (h + 1) * blk],
                va[h // 2, (h % 2) * lat_w : (h % 2 + 1) * lat_w, :],
                preferred_element_type=F32,
            )
            gain = hgs[h // 2, h % 2 : h % 2 + 1].astype(F32)
            ho[b * blk : (b + 1) * blk, h * 128 : (h + 1) * 128] = rms(v, gain).astype(BF16)
        if b == 0:
            pl.when(first_two)(pass_out)
            for j in range(len(near), nj):
                pass_on(3, j)

    own_cps[3].wait()
    for j in range(nj):
        collect(3, j)
    wide = min(512, out.shape[1])
    tiles = out.shape[1] // wide

    def out_cp(t):
        at = pl.ds(pl.multiple_of(t * wide, wide), wide)
        return pltpu.make_async_copy(res.at[:, at], out.at[:, at], out_sem.at[t])

    def finish(t, _):
        at = pl.ds(pl.multiple_of(t * wide, wide), wide)
        total = jnp.zeros((2 * blk, wide), F32)
        for g in range(ny):
            part = jnp.dot(ho[:, g * 256 : (g + 1) * 256], wo[g, :, at], preferred_element_type=F32)
            total = total + part.astype(BF16).astype(F32)
        res[:, at] = total.astype(BF16)
        out_cp(t).start()
        return 0

    lax.fori_loop(0, tiles, finish, 0, unroll=True)
    flush(late)
    for t in range(tiles):
        out_cp(t).wait()


def body(dims, tokens, query_weight, latent_weight, key_absorb, query_gain, latent_gain, value_absorb, head_gain, out_weight, chosen):
    nz, nx, nc, ny, nsel, nloc = dims
    np_, sb, nr = nx * nc, 2 * ny, nsel - nloc
    rows, d = tokens.shape
    heads, hd, lat_w = key_absorb.shape
    blk = rows // 2
    sh = blk // ny
    rsteps = nz // 2
    any_ = pl.BlockSpec(memory_space=pl.ANY)
    dma = pltpu.SemaphoreType.DMA
    piece = pltpu.VMEM((sb, sh, lat_w), BF16)
    scratch = [
        pltpu.SMEM((sb, nsel), jnp.int32),
        pltpu.VMEM((lat_w,), BF16),
        pltpu.VMEM((lat_w,), BF16),
        pltpu.VMEM((rows, d), BF16),
        pltpu.VMEM((d, lat_w), BF16),
        pltpu.VMEM((ny, d, heads * hd), BF16),
        pltpu.VMEM((ny, heads * hd, d), BF16),
        pltpu.VMEM((ny, heads * hd, lat_w), BF16),
        pltpu.VMEM((ny, heads * lat_w, hd), BF16),
        pltpu.VMEM((ny, heads, hd), BF16),
        pltpu.VMEM((2, ny, sh, lat_w), BF16),
        pltpu.VMEM((sb, ny, sh, lat_w), BF16),
        piece,
        pltpu.VMEM((np_, 8, 128), jnp.int32),
        pltpu.VMEM((np_, 8, 128), jnp.int32),
        pltpu.SMEM((np_, 8, 128), jnp.int32),
        pltpu.VMEM((np_ * nz, sh, lat_w), BF16),
        pltpu.VMEM((np_ * nz, sh, lat_w), BF16),
        pltpu.VMEM((ny - 1, 2, nr, sh, lat_w), BF16),
        pltpu.VMEM((2, nsel, ny, sh, lat_w), BF16),
        pltpu.VMEM((2, 2 * ny * blk, lat_w), BF16),
        pltpu.VMEM((2, 8, nsel * blk), jnp.int32),
        pltpu.VMEM((2 * ny * blk, lat_w), BF16),
        pltpu.VMEM((rows, heads * ny * hd), BF16),
        dma((11,)),
        dma((4,)), dma((4,)),
        dma((rsteps + 4,)), dma((rsteps, CUTS)), dma((rsteps + 4,)), dma((rsteps, CUTS)),
        dma((10,)), dma((10,)),
        dma((2,)), dma((2,)),
        dma((5, 4)), dma((4, 3)), dma((4, 3)), dma((4, 3, 2)),
        pltpu.VMEM((rows, d), BF16), dma((4,)), pltpu.SemaphoreType.REGULAR,
    ] + [piece] * (nz - 1)
    return pl.pallas_call(
        functools.partial(kernel, dims),
        out_shape=jax.ShapeDtypeStruct((rows, d), BF16),
        in_specs=[any_] * 10,
        out_specs=any_,
        scratch_shapes=scratch,
        compiler_params=pltpu.CompilerParams(
            collective_id=0, has_side_effects=True, vmem_limit_bytes=60 * 2**20
        ),
        name="attend",
    )(
        chosen,
        tokens,
        latent_weight,
        query_weight,
        key_absorb.reshape(heads * hd, lat_w),
        value_absorb.reshape(heads * lat_w, hd),
        out_weight,
        head_gain,
        query_gain,
        latent_gain,
    )


def build(devices, dims):
    nz, nx, nc, ny = dims[:4]
    finer = Mesh(devices.reshape(nz, nx, nc, ny), KV_TP)
    in_specs = (
        P(KV_TP, None),
        P(None, "tp"),
        P(),
        P("tp", None, None),
        P(),
        P(),
        P("tp", None, None),
        P("tp", None),
        P("tp", None),
        P(KV, None),
    )
    return jax.shard_map(
        functools.partial(body, dims), mesh=finer, in_specs=in_specs, out_specs=P(KV_TP, None), check_vma=False
    )


def solution(mesh):
    return build(mesh.devices, (16, 4, 2, mesh.shape["tp"], 16, 4))
```

```python
import functools

import jax
import jax.numpy as jnp
from jax import lax
from jax.experimental import pallas as pl
from jax.experimental.pallas import tpu as pltpu
from jax.sharding import Mesh
from jax.sharding import PartitionSpec as P

KV = ("kv_0", "kv_1", "kv_2")
KV_TP = ("kv_0", "kv_1", "kv_2", "tp")
MESH = pl.DeviceIdType.MESH
EPS = 1e-06
BF16 = jnp.bfloat16
F32 = jnp.float32
LOG2E = 1.4426950408889634
CUTS = 4


def rms(v, gain):
    return v * lax.rsqrt(jnp.mean(v * v, axis=-1, keepdims=True) + EPS) * gain


def kernel(
    dims,
    chosen_hbm,
    tokens_hbm,
    lw_hbm,
    qw_hbm,
    ka_hbm,
    va_hbm,
    ow_hbm,
    hg,
    qg_hbm,
    lg_hbm,
    out,
    *scratch,
):
    nz, nx, nc, ny, nsel, nloc = dims
    np_ = nx * nc
    sb = 2 * ny
    nr = nsel - nloc
    rsteps = nz // 2
    lsteps = nz - 1 - rsteps
    (
        chosen, qg, lg, tok, lw, wq, wo, ka, va, hgs, lat, span, piece0, want, wt, wts,
        xs, xr, ys, kvb, ab, kp, mix, ho,
        loc_sem, small_s, small_r, r_s, r_r, l_s, l_r,
        x_s, x_r, y_s, y_r, w_s, w1_r, w2_r, w3_r, res, out_sem, ready,
        *ring,
    ) = scratch
    right = [piece0] + list(ring[:rsteps])
    left = [piece0] + list(ring[rsteps:])
    sh = piece0.shape[1]
    lat_w = piece0.shape[2]
    blk = sh * ny

    z = lax.axis_index("kv_0")
    x = lax.axis_index("kv_1")
    c = lax.axis_index("kv_2")
    y = lax.axis_index("tp")
    xc = x * nc + c

    def at_plane(d):
        p = lax.rem(xc + d + np_, np_)
        return {"kv_1": lax.div(p, nc), "kv_2": lax.rem(p, nc)}

    def at_y(e):
        return {"tp": lax.rem(y + e + ny, ny)}

    def at_z(d):
        return {"kv_0": lax.rem(z + d + nz, nz)}

    def at_x(d):
        return {"kv_1": lax.rem(x + d + nx, nx)}

    def when(cond, f):
        if cond is None:
            f()
        else:
            pl.when(cond)(f)

    def remote(src, dst, s, r, dev):
        return pltpu.make_async_remote_copy(
            src_ref=src, dst_ref=dst, send_sem=s, recv_sem=r,
            device_id=dev, device_id_type=MESH,
        )

    def send(src, dst, s, r, dev, cond=None):
        when(cond, remote(src, dst, s, r, dev).start)

    def arrive(ref, r, cond=None):
        when(cond, remote(ref, ref, loc_sem.at[0], r, at_y(1)).wait_recv)

    drains, late = [], []

    def drain(ref, s, cond=None, to=drains):
        to.append((cond, remote(ref, ref, s, loc_sem.at[0], at_y(1))))

    def flush(queue):
        for cond, cp in queue:
            when(cond, cp.wait_send)
        queue.clear()

    tok_cp = pltpu.make_async_copy(tokens_hbm, tok, loc_sem.at[0])
    lw_cp = pltpu.make_async_copy(lw_hbm, lw, loc_sem.at[1])
    own_cps = [
        pltpu.make_async_copy(qw_hbm, wq.at[y], loc_sem.at[2]),
        pltpu.make_async_copy(ka_hbm, ka.at[y], loc_sem.at[3]),
        pltpu.make_async_copy(va_hbm, va.at[y], loc_sem.at[4]),
        pltpu.make_async_copy(ow_hbm, wo.at[y], loc_sem.at[5]),
    ]
    small_cps = [
        pltpu.make_async_copy(chosen_hbm, chosen, loc_sem.at[7]),
        pltpu.make_async_copy(lg_hbm, lg, loc_sem.at[8]),
        pltpu.make_async_copy(qg_hbm, qg, loc_sem.at[9]),
        pltpu.make_async_copy(hg, hgs.at[y], loc_sem.at[10]),
    ]
    for cp in [tok_cp, lw_cp] + small_cps:
        cp.start()

    split = nz > 4
    offsets = sorted({1 % nz, 2 % nz, (nz - 1) % nz, (nz - 2) % nz} - {0})
    barrier = pltpu.get_barrier_semaphore()
    peers = [(at_y(e), None) for e in range(1, ny)]
    peers += [(at_z(d), z + d < nz if split and d < 3 else None) for d in offsets]
    peers += [(at_plane(d), None) for d in range(1, np_)]

    def greet(sem, dev):
        pl.semaphore_signal(sem, inc=1, device_id=dev, device_id_type=MESH)

    for dev, cond in peers:
        when(cond, functools.partial(greet, barrier, dev))

    def enter():
        if not split:
            pl.semaphore_wait(barrier, len(peers))
            return
        for k, cond in ((0, z >= 2), (1, z == 1), (2, z == 0)):
            pl.when(cond)(functools.partial(pl.semaphore_wait, barrier, len(peers) - k))
        for d in (1, 2):
            pl.when(z + d >= nz)(functools.partial(greet, ready, at_z(d)))

    def wait_wrap():
        if split:
            pl.when(z == 0)(functools.partial(pl.semaphore_wait, ready, 2))
            pl.when(z == 1)(functools.partial(pl.semaphore_wait, ready, 1))

    xs[...] = jnp.zeros_like(xs)
    xr[...] = jnp.zeros_like(xr)

    d_io = lax.broadcasted_iota(jnp.int32, (8, 128), 0)
    i_io = lax.broadcasted_iota(jnp.int32, (8, 128), 1)
    owner_of = lax.rem(z - lax.rem(i_io, nz) + nz, nz) * np_ + lax.rem(
        xc - lax.rem(d_io, np_) + np_, np_
    )
    acc = jnp.zeros((8, 128), jnp.int32)
    small_cps[0].wait()
    for row in range(sb):
        for p in range(nloc, nsel):
            v = chosen[row, p]
            acc = jnp.where(owner_of == lax.div(v, sb), lax.rem(v, sb), acc)
    for d in range(np_):
        row = jnp.broadcast_to(acc[d : d + 1], (8, 128))
        if d == 0:
            wt[0] = row
        else:
            want[d] = row

    small_cps[1].wait()
    tok_cp.wait()
    lw_cp.wait()
    for cp in own_cps:
        cp.start()
    values = jnp.dot(tok[...], lw[...], preferred_element_type=F32)
    latent = rms(values, lg[...].astype(F32).reshape(1, lat_w)).astype(BF16).reshape(2, ny, sh, lat_w)
    lat[...] = latent
    span[pl.ds(2 * y, 2)] = latent
    piece0[pl.ds(2 * y, 2)] = lat[:, y]

    far_y = sorted(range(1, ny), key=lambda e: -min(e, ny - e))
    far_x = sorted(range(1, np_), key=lambda d: -min(d, np_ - d))
    enter()

    for e in far_y:
        send(lat.at[:, lax.rem(y + e, ny)], piece0.at[pl.ds(2 * y, 2)], small_s.at[0], small_r.at[0], at_y(e))
    for d in range(1, np_):
        send(want.at[d], wt.at[d], small_s.at[1], small_r.at[1], at_plane(-d))
    others = piece0.at[pl.ds(0, 2 * (ny - 1))]
    drain(others, small_s.at[0])
    drain(wt.at[pl.ds(1, np_ - 1)], small_s.at[1])

    big = [(qw_hbm, wq), (ka_hbm, ka), (va_hbm, va), (ow_hbm, wo)]
    parts = 2 * nc
    near = [1, ny - 1] if ny > 2 else [1]
    nj = ny - 1
    shard_of = [lax.rem(y - e + ny, ny) for e in near]
    if ny > 2:
        shard_of.append(lax.rem(y + 2, ny))
    mate = {"kv_2": 1 - c}

    def rows_of(a, far=False, half=None):
        par = lax.rem(x if a < 3 else z, 2)
        g = (1 - par if far else par) * nc + c
        n = big[a][0].shape[0] // parts
        if half is None:
            return pl.ds(pl.multiple_of(g * n, n), n)
        return pl.ds(pl.multiple_of(g * n + half * (n // 2), n // 2), n // 2)

    def shares(a, k):
        n = big[a][0].shape[0] // parts
        return big[a][1].at[pl.ds(0, nj), pl.ds(0, k * n)]

    def launch(a):
        for j, e in enumerate(near):
            send(big[a][0].at[rows_of(a)], big[a][1].at[y, rows_of(a)], w_s.at[0, a], w1_r.at[a, j], at_y(e))
        drain(shares(a, 1), w_s.at[0, a], to=late)
        if a < 3:
            drain(shares(a, 1), w_s.at[1, a], to=late)
        else:
            n = big[a][0].shape[0] // parts // 2
            halves = big[a][1].at[pl.ds(0, nj), pl.ds(0, n)]
            drain(halves, w_s.at[1, a], to=late)
            drain(halves, w_s.at[3, a], z < nz - 1, to=late)
            drain(halves, w_s.at[4, a], z == 1, to=late)
        if nc > 1:
            drain(shares(a, 2), w_s.at[2, a], to=late)

    def forward(a):
        w = big[a][1]
        for j in range(len(near)):
            arrive(w.at[shard_of[j], rows_of(a)], w1_r.at[a, j])
            if ny > 2:
                part = w.at[shard_of[j], rows_of(a, half=j)]
                send(part, part, w_s.at[0, a], w1_r.at[a, 2], at_y(near[j]))

    def spread(a, j):
        w = big[a][1]
        mine = w.at[shard_of[j], rows_of(a)]
        if j == 2:
            arrive(mine, w1_r.at[a, 2])
        lo, hi = (w.at[shard_of[j], rows_of(a, half=half)] for half in (0, 1))
        if a < 3:
            send(lo, lo, w_s.at[1, a], w2_r.at[a, j], at_x(1))
            send(hi, hi, w_s.at[1, a], w2_r.at[a, j], at_x(-1))
        else:
            send(hi, hi, w_s.at[1, a], w2_r.at[a, j], at_z(-1))
            send(lo, lo, w_s.at[3, a], w2_r.at[a, j], at_z(1), z < nz - 1)
            send(lo, lo, w_s.at[4, a], w2_r.at[a, j], at_z(-1), z == 1)
        if nc > 1:
            send(mine, mine, w_s.at[2, a], w3_r.at[a, j, 0], mate)

    def pass_on(a, j):
        far = big[a][1].at[shard_of[j], rows_of(a, far=True)]
        arrive(far, w2_r.at[a, j])
        if nc > 1:
            send(far, far, w_s.at[2, a], w3_r.at[a, j, 1], mate)

    def collect(a, j):
        if nc > 1:
            slice_ = big[a][1].at[0, pl.ds(0, big[a][0].shape[0] // parts)]
            arrive(slice_, w3_r.at[a, j, 0])
            arrive(slice_, w3_r.at[a, j, 1])

    for a in range(3):
        launch(a)

    arrive(others, small_r.at[0])

    def targets(s, steps):
        ts = [1] if s < 2 else ([2, 1] if s % 2 == 0 else [])
        return [t for t in ts if s + t <= steps]

    cut = sb // CUTS
    r_hops = [(s, t) for s in range(rsteps) for t in targets(s, rsteps)]
    l_hops = [(s, t) for s in range(lsteps) for t in targets(s, lsteps)]

    def r_cond(s, t):
        return jnp.logical_and(z >= s, z + t <= nz - 1)

    def l_cond(s):
        return lax.rem(z + s, nz) < lsteps

    def hop_right(s, k):
        at = pl.ds(k * cut, cut)
        for t in targets(s, rsteps):
            h = r_hops.index((s, t))
            send(right[s].at[at], right[s + t].at[at], r_s.at[h], r_r.at[s + t - 1, k], at_z(t), r_cond(s, t))

    def hop_left(s, k, cond=None):
        at = pl.ds(k * cut, cut)
        for t in targets(s, lsteps):
            h = l_hops.index((s, t))
            ok = l_cond(s) if cond is None else cond
            send(left[s].at[at], left[s + t].at[at], l_s.at[h], l_r.at[s + t - 1, k], at_z(-t), ok)

    for k in range(CUTS):
        hop_right(0, k)
        hop_left(0, k, jnp.logical_and(l_cond(0), z > 0) if split else None)
    for h, (s, t) in enumerate(r_hops):
        drain(right[s], r_s.at[h], r_cond(s, t))
    for h, (s, t) in enumerate(l_hops):
        drain(left[s], l_s.at[h], l_cond(s))

    arrive(wt.at[pl.ds(1, np_ - 1)], small_r.at[1])
    wt_cp = pltpu.make_async_copy(wt, wts, loc_sem.at[6])
    wt_cp.start()
    wt_cp.wait()

    def select(ref, i):
        for d in range(np_):
            block = ref[wts[d, 0, i]]
            if d == 0:
                xr[i] = block
            else:
                xs[d * nz + i] = block

    groups = []

    def post(lo, n, cond):
        k = len(groups)
        groups.append((n, cond))
        for d in far_x:
            at = pl.ds(d * nz + lo, n)
            send(xs.at[at], xr.at[at], x_s.at[k], x_r.at[k], at_plane(d), cond)
        drain(xs.at[pl.ds(0, (np_ - 1) * n)], x_s.at[k], cond)

    def take(s):
        for k in range(CUTS):
            at = pl.ds(k * cut, cut)
            arrive(right[s].at[at], r_r.at[s - 1, k], z >= s)
            if s < rsteps:
                hop_right(s, k)
            if s <= lsteps:
                arrive(left[s].at[at], l_r.at[s - 1, k], l_cond(s))
                if s < lsteps:
                    hop_left(s, k)

    early = z < nz // 2
    first_two = z < min(2, nz // 2)
    middle = jnp.logical_and(early, z >= 2)

    def spread_out():
        for j in range(len(near)):
            spread(3, j)

    def spread_two():
        for a in range(3):
            spread(a, 2)

    def first_planes():
        if nj > 2:
            spread_two()
        forward(3)
        spread_out()

    def first_weights():
        forward(0)
        for j in range(len(near)):
            spread(0, j)

    def pass_out():
        for j in range(len(near)):
            pass_on(3, j)

    select(piece0, 0)
    pl.when(first_two)(first_weights)
    wait_wrap()
    if split:
        for k in range(CUTS):
            hop_left(0, k, z == 0)
    r_lo, l_hi = 0, nz
    stages = [[1], [2]] + [[s + 1, s] for s in range(3, nz, 2)]
    for stage in stages:
        stage = [s for s in stage if s <= rsteps]
        if not stage:
            continue
        for s in stage:
            take(s)
        for s in stage:
            pl.when(z >= s)(functools.partial(select, right[s], s))
            if s <= lsteps:
                pl.when(z + s >= nz)(functools.partial(select, left[s], nz - s))
        top = max(stage)
        if top > 1 or top == rsteps:
            post(r_lo, top + 1 - r_lo, z >= r_lo)
            r_lo = top + 1
            l_top = min(top, lsteps)
            if nz - l_top < l_hi:
                post(nz - l_top, l_hi - (nz - l_top), z + l_top >= nz)
                l_hi = nz - l_top
        if 1 in stage:
            pl.when(jnp.logical_not(first_two))(first_weights)
        if 2 in stage or rsteps < 2:
            for a in (1, 2):
                forward(a)
                for j in range(len(near)):
                    spread(a, j)
            launch(3)
        if 4 in stage:
            pl.when(first_two)(first_planes)
            if nj > 2:
                pl.when(middle)(spread_two)
        if 6 in stage:
            pl.when(jnp.logical_not(first_two))(functools.partial(forward, 3))
            pl.when(middle)(spread_out)
    if rsteps < 4:
        pl.when(first_two)(first_planes)
        if nj > 2:
            pl.when(middle)(spread_two)
    if rsteps < 6:
        pl.when(jnp.logical_not(first_two))(functools.partial(forward, 3))
        pl.when(middle)(spread_out)
    for e in range(1, ny):
        send(lat, span.at[pl.ds(2 * y, 2)], small_s.at[2], small_r.at[2], at_y(e))
        send(hg, hgs.at[y], small_s.at[3], small_r.at[3], at_y(e))
    drain(span.at[pl.ds(0, 2 * (ny - 1))], small_s.at[2])
    drain(hgs.at[pl.ds(0, ny - 1)], small_s.at[3])

    pl.when(jnp.logical_not(early))(spread_out)
    for a in range(3):
        for j in range(len(near)):
            pass_on(a, j)
    if nj > 2:
        spread(3, 2)

    for k, (n, cond) in enumerate(groups):
        if k == max(0, len(groups) - 2) and nj > 2:
            pl.when(jnp.logical_not(early))(spread_two)
        arrive(xr.at[pl.ds(0, (np_ - 1) * n)], x_r.at[k], cond)

    for b in range(2):
        for e in far_y + [0]:
            row = 2 * lax.rem(y + e, ny) + b
            for j in range(nr):
                o = lax.div(chosen[row, nloc + j], sb)
                i = lax.rem(z - lax.div(o, np_) + nz, nz)
                d = lax.rem(xc - lax.rem(o, np_) + np_, np_)
                block = xr[d * nz + i]
                if e == 0:
                    kvb[b, nloc + j, y] = block
                else:
                    ys[e - 1, b, j] = block
            if e:
                send(ys.at[e - 1, b], kvb.at[b, pl.ds(nloc, nr), y], y_s.at[b], y_r.at[b], at_y(e))
        drain(ys.at[:, b], y_s.at[b], to=late)
    arrive(span.at[pl.ds(0, 2 * (ny - 1))], small_r.at[2])
    arrive(hgs.at[pl.ds(0, ny - 1)], small_r.at[3])
    lane = lax.broadcasted_iota(jnp.int32, (8, 128), 1)
    first = ((z * nx + x) * nc + c) * sb
    for b in range(2):
        row = 2 * y + b
        for p in range(nloc):
            kvb[b, p] = span[lax.rem(chosen[row, p], sb)]
        for p in range(0, nsel, 2):
            base = jnp.where(lane < blk, chosen[row, p] * blk, chosen[row, p + 1] * blk - blk)
            kp[b, :, p * blk : (p + 2) * blk] = base + lane

    small_cps[2].wait()
    small_cps[3].wait()
    for cp in own_cps[:3]:
        cp.wait()
    for j in range(len(near)):
        for a in range(3):
            collect(a, j)

    def project(g):
        q = jnp.dot(tok[...], wq[g], preferred_element_type=F32).astype(BF16)
        for hh in range(2):
            a = jnp.dot(q[:, hh * 128 : (hh + 1) * 128], ka[g, hh * 128 : (hh + 1) * 128, :], preferred_element_type=F32)
            a = rms(a, qg[...].astype(F32).reshape(1, lat_w)).astype(BF16)
            at = pl.ds(pl.multiple_of((2 * g + hh) * blk, blk), blk)
            ab[0, at] = a[:blk]
            ab[1, at] = a[blk:]

    def project_near(i, _):
        project(lax.rem(y + ny + lax.rem(i + 1, 3) - 1, ny))
        return 0

    lax.fori_loop(0, len(near) + 1, project_near, 0)
    flush(drains)
    pl.when(jnp.logical_not(first_two))(pass_out)
    if nj > 2:
        for a in range(3):
            pass_on(a, 2)
        for a in range(3):
            collect(a, 2)
        project(shard_of[2])

    chunk = min(4, 2 * ny) * blk
    for b in range(2):
        arrive(ys.at[:, b], y_r.at[b])
        keys = kvb[b].reshape(nsel * blk, lat_w)
        q_pos = (first + 2 * y + b) * blk + lax.rem(
            lax.broadcasted_iota(jnp.int32, (chunk, nsel * blk), 0), blk
        )
        seen = kp[b, 0:1, :] <= q_pos
        for i in range(2 * ny * blk // chunk):
            sc = lax.dot_general(
                ab[b, i * chunk : (i + 1) * chunk], keys, (((1,), (1,)), ((), ())),
                preferred_element_type=F32,
            )
            sc = jnp.where(seen, sc, -jnp.inf)
            top = jnp.max(sc, axis=-1, keepdims=True)
            ex = jnp.exp2((sc - top) * (LOG2E * lat_w ** (-0.5)))
            wgt = (ex * (1.0 / jnp.sum(ex, axis=-1, keepdims=True))).astype(BF16)
            mix[i * chunk : (i + 1) * chunk] = jnp.dot(
                wgt, keys, preferred_element_type=F32
            ).astype(BF16)
        for h in range(2 * ny):
            v = jnp.dot(
                mix[h * blk : (h + 1) * blk],
                va[h // 2, (h % 2) * lat_w : (h % 2 + 1) * lat_w, :],
                preferred_element_type=F32,
            )
            gain = hgs[h // 2, h % 2 : h % 2 + 1].astype(F32)
            ho[b * blk : (b + 1) * blk, h * 128 : (h + 1) * 128] = rms(v, gain).astype(BF16)
        if b == 0:
            pl.when(first_two)(pass_out)
            for j in range(len(near), nj):
                pass_on(3, j)

    own_cps[3].wait()
    for j in range(nj):
        collect(3, j)
    wide = min(512, out.shape[1])
    tiles = out.shape[1] // wide

    def out_cp(t):
        at = pl.ds(pl.multiple_of(t * wide, wide), wide)
        return pltpu.make_async_copy(res.at[:, at], out.at[:, at], out_sem.at[t])

    def finish(t, _):
        at = pl.ds(pl.multiple_of(t * wide, wide), wide)
        total = jnp.zeros((2 * blk, wide), F32)
        for g in range(ny):
            part = jnp.dot(ho[:, g * 256 : (g + 1) * 256], wo[g, :, at], preferred_element_type=F32)
            total = total + part.astype(BF16).astype(F32)
        res[:, at] = total.astype(BF16)
        out_cp(t).start()
        return 0

    lax.fori_loop(0, tiles, finish, 0, unroll=True)
    flush(late)
    for t in range(tiles):
        out_cp(t).wait()


def body(dims, tokens, query_weight, latent_weight, key_absorb, query_gain, latent_gain, value_absorb, head_gain, out_weight, chosen):
    nz, nx, nc, ny, nsel, nloc = dims
    np_, sb, nr = nx * nc, 2 * ny, nsel - nloc
    rows, d = tokens.shape
    heads, hd, lat_w = key_absorb.shape
    blk = rows // 2
    sh = blk // ny
    rsteps = nz // 2
    any_ = pl.BlockSpec(memory_space=pl.ANY)
    dma = pltpu.SemaphoreType.DMA
    piece = pltpu.VMEM((sb, sh, lat_w), BF16)
    scratch = [
        pltpu.SMEM((sb, nsel), jnp.int32),
        pltpu.VMEM((lat_w,), BF16),
        pltpu.VMEM((lat_w,), BF16),
        pltpu.VMEM((rows, d), BF16),
        pltpu.VMEM((d, lat_w), BF16),
        pltpu.VMEM((ny, d, heads * hd), BF16),
        pltpu.VMEM((ny, heads * hd, d), BF16),
        pltpu.VMEM((ny, heads * hd, lat_w), BF16),
        pltpu.VMEM((ny, heads * lat_w, hd), BF16),
        pltpu.VMEM((ny, heads, hd), BF16),
        pltpu.VMEM((2, ny, sh, lat_w), BF16),
        pltpu.VMEM((sb, ny, sh, lat_w), BF16),
        piece,
        pltpu.VMEM((np_, 8, 128), jnp.int32),
        pltpu.VMEM((np_, 8, 128), jnp.int32),
        pltpu.SMEM((np_, 8, 128), jnp.int32),
        pltpu.VMEM((np_ * nz, sh, lat_w), BF16),
        pltpu.VMEM((np_ * nz, sh, lat_w), BF16),
        pltpu.VMEM((ny - 1, 2, nr, sh, lat_w), BF16),
        pltpu.VMEM((2, nsel, ny, sh, lat_w), BF16),
        pltpu.VMEM((2, 2 * ny * blk, lat_w), BF16),
        pltpu.VMEM((2, 8, nsel * blk), jnp.int32),
        pltpu.VMEM((2 * ny * blk, lat_w), BF16),
        pltpu.VMEM((rows, heads * ny * hd), BF16),
        dma((11,)),
        dma((4,)), dma((4,)),
        dma((rsteps + 4,)), dma((rsteps, CUTS)), dma((rsteps + 4,)), dma((rsteps, CUTS)),
        dma((10,)), dma((10,)),
        dma((2,)), dma((2,)),
        dma((5, 4)), dma((4, 3)), dma((4, 3)), dma((4, 3, 2)),
        pltpu.VMEM((rows, d), BF16), dma((4,)), pltpu.SemaphoreType.REGULAR,
    ] + [piece] * (nz - 1)
    return pl.pallas_call(
        functools.partial(kernel, dims),
        out_shape=jax.ShapeDtypeStruct((rows, d), BF16),
        in_specs=[any_] * 10,
        out_specs=any_,
        scratch_shapes=scratch,
        compiler_params=pltpu.CompilerParams(
            collective_id=0, has_side_effects=True, vmem_limit_bytes=60 * 2**20
        ),
        name="attend",
    )(
        chosen,
        tokens,
        latent_weight,
        query_weight,
        key_absorb.reshape(heads * hd, lat_w),
        value_absorb.reshape(heads * lat_w, hd),
        out_weight,
        head_gain,
        query_gain,
        latent_gain,
    )


def build(devices, dims):
    nz, nx, nc, ny = dims[:4]
    finer = Mesh(devices.reshape(nz, nx, nc, ny), KV_TP)
    in_specs = (
        P(KV_TP, None),
        P(None, "tp"),
        P(),
        P("tp", None, None),
        P(),
        P(),
        P("tp", None, None),
        P("tp", None),
        P("tp", None),
        P(KV, None),
    )
    return jax.shard_map(
        functools.partial(body, dims), mesh=finer, in_specs=in_specs, out_specs=P(KV_TP, None), check_vma=False
    )


def solution(mesh):
    return build(mesh.devices, (16, 4, 2, mesh.shape["tp"], 16, 4))
```
